256 devices in a mesh: sp: 32 (over z, y), tp: 8 (over x, core).
Axes of the slice: x: 4, y: 4, z: 8, core: 2. Of those that a mesh axis runs over, the one named last changes fastest.
Arguments:
- tokens: bfloat16 [16384, 2048], P('sp', 'tp'), may hold values from -400 to 400
- norm_gain: float32 [2048], replicated, may hold values from 0.1 to 1.9
- query_weight: bfloat16 [2048, 1024], P(None, 'tp'), may hold values from -0.37306796 to 0.37306796
- key_weight: bfloat16 [2048, 1024], P(None, 'tp'), may hold values from -0.2625825 to 0.2625825
- value_weight: bfloat16 [2048, 1024], P(None, 'tp'), may hold values from -0.125 to 0.125
- outer_gate_weight: bfloat16 [2048, 1024], P(None, 'tp'), may hold values from -0.125 to 0.125
- inner_gate_weight: bfloat16 [2048, 1024], P(None, 'tp'), may hold values from -0.125 to 0.125
- conv_input_weight: bfloat16 [2048, 1024], P(None, 'tp'), may hold values from -0.125 to 0.125
- conv_taps: float32 [3, 1024], P(None, 'tp'), may hold values from -3.5 to 3.5
- lambdas: float32 [8], P('tp'), may hold values from 0.3 to 0.8
- head_gain: float32 [128], replicated, may hold values from 0.1 to 1.9
- attn_out_weight: bfloat16 [1024, 2048], P(None, 'tp'), may hold values from -0.125 to 0.125
- conv_out_weight: bfloat16 [1024, 2048], P(None, 'tp'), may hold values from -0.125 to 0.125
Outputs:
- mixed_out: bfloat16 [16384, 2048], P('sp', 'tp')
- log_totals: float32 [8, 2, 16384], P('tp', None, 'sp')
The draws below stay inside these ranges and needn't reach their ends.
All inputs are finite; a program needn't handle non-finite values.
Results may differ from the reference program's by a relative error of at most 0.014.
The reference program's roundings to bfloat16 on the way count: a program that leaves them out, or rounds other values in their place, can miss the bound.
Values may be sent and summed in bfloat16 or wider, within the bound.
A program may use at most 128 MiB of HBM per device.

```python
import jax
import jax.numpy as jnp
from jax import lax

WIDTH = 2048
HEADS = 8
HEAD_DIM = 64
TAPS = 3
TOK_DEV = 512
CHANNELS = 1024
TOKENS = 16384


def drawn_weight(key, salt, fan_in):
    base = jax.random.normal(jax.random.fold_in(key, salt), (WIDTH, CHANNELS), jnp.float32)
    base = jnp.clip(base, -6.0, 6.0) * fan_in ** (-0.5)
    return base.astype(jnp.bfloat16)


def draw_query_weight(key, part):
    return drawn_weight(key, 11, WIDTH / 3.0)


def draw_key_weight(key, part):
    return drawn_weight(key, 12, WIDTH * 1.0)


def draw_tokens(key, part):
    values = jnp.clip(jax.random.normal(jax.random.fold_in(key, 2), (TOKENS, WIDTH), jnp.float32), -6.0, 6.0)
    return values.astype(jnp.bfloat16)


def level_of(stream_key, shape, split, low, largest):
    def one(position, parts):
        heights = jax.random.uniform(jax.random.fold_in(jax.random.fold_in(stream_key, 6), position), (parts,), jnp.float32, low / len(split), largest / len(split))
        return jnp.repeat(jnp.exp(heights), shape[position] // parts).reshape((-1,) + (1,) * (len(shape) - position - 1))

    level = one(*split[0])
    for cut in split[1:]:
        level = level * one(*cut)
    return level


def centred(key, dims, spread, most, split=(), held_as=jnp.bfloat16):
    array = jax.random.normal(key, dims, jnp.float32) * spread
    if len(split) > 0:
        array = level_of(key, dims, split, -0.22, 0.18) * array
    return jnp.clip(array, min=-most, max=most).astype(held_as)


def setup_inputs(seed: int = 0) -> dict:
    streams_of = jax.random.split(jax.random.key(seed), 14)
    return {
        "tokens": draw_tokens(jax.random.fold_in(streams_of[13], 71), 0),
        "norm_gain": jnp.clip(1.0 + 0.18 * jax.random.normal(streams_of[1], (WIDTH,), jnp.float32), 0.1, 1.9),
        "query_weight": draw_query_weight(jax.random.fold_in(streams_of[13], 71), 0),
        "key_weight": draw_key_weight(jax.random.fold_in(streams_of[13], 71), 0),
        "value_weight": centred(streams_of[4], (WIDTH, CHANNELS), WIDTH ** -0.5, 0.125, ((1, 8),)),
        "outer_gate_weight": centred(streams_of[5], (WIDTH, CHANNELS), WIDTH ** -0.5, 0.125, ((1, 8),)),
        "inner_gate_weight": centred(streams_of[6], (WIDTH, CHANNELS), WIDTH ** -0.5, 0.125, ((1, 8),)),
        "conv_input_weight": centred(streams_of[7], (WIDTH, CHANNELS), WIDTH ** -0.5, 0.125, ((1, 8),)),
        "conv_taps": centred(streams_of[8], (TAPS, CHANNELS), TAPS ** -0.5, 3.5, ((1, 8),), jnp.float32),
        "lambdas": jnp.clip(0.3 + 0.5 * jax.random.uniform(streams_of[9], (HEADS,), jnp.float32) ** level_of(streams_of[9], (HEADS,), ((0, 8),), -0.2, 0.2), 0.3, 0.8),
        "head_gain": jnp.clip(1.0 + 0.18 * jax.random.normal(streams_of[10], (2 * HEAD_DIM,), jnp.float32), 0.1, 1.9),
        "attn_out_weight": centred(streams_of[11], (CHANNELS, WIDTH), (2 * CHANNELS) ** -0.5, 0.125, ((1, 8),)),
        "conv_out_weight": centred(streams_of[12], (CHANNELS, WIDTH), (2 * CHANNELS) ** -0.5, 0.125, ((1, 8),)),
    }


NORM_EPS = 1e-06
HEAD_EPS = 1e-05
ROPE_BASE = 500000.0
MASKED = -1e+30
HEAD_SCALE = 0.8

def rotate(field_in, positions):
    half_dim = field_in.shape[-1] // 2
    frequency = ROPE_BASE ** (-jnp.arange(half_dim, dtype=jnp.float32) * 2.0 / field_in.shape[-1])
    angles = positions[:, None] * frequency[None, :]
    cosine = jnp.cos(angles)[:, None, None, :]
    sine_part = jnp.sin(angles)[:, None, None, :]
    first_half = field_in[..., :half_dim]
    second_half = field_in[..., half_dim:]
    return jnp.concatenate([first_half * cosine - second_half * sine_part, second_half * cosine + first_half * sine_part], axis=-1)

def reference(tokens, norm_gain, query_weight, key_weight, value_weight, outer_gate_weight, inner_gate_weight, conv_input_weight, conv_taps, lambdas, head_gain, attn_out_weight, conv_out_weight):
    floats = tokens.astype(jnp.float32)
    inverse_rms = lax.rsqrt(lax.optimization_barrier(jnp.mean(floats * floats, axis=1, keepdims=True)) + NORM_EPS)
    scaled = (floats * norm_gain[None, :]).astype(jnp.bfloat16)

    def project(weight):
        return inverse_rms * jnp.dot(scaled, weight, preferred_element_type=jnp.float32)
    positions = jnp.arange(TOKENS, dtype=jnp.float32)
    queries = rotate(project(query_weight).reshape(TOKENS, HEADS, 2, HEAD_DIM), positions).astype(jnp.bfloat16)
    key_rows = rotate(project(key_weight).reshape(TOKENS, HEADS, 2, HEAD_DIM), positions).astype(jnp.bfloat16)
    values = project(value_weight).astype(jnp.bfloat16).reshape(TOKENS, HEADS, 2 * HEAD_DIM)
    outer_gate = project(outer_gate_weight).astype(jnp.bfloat16)
    inner_gate = project(inner_gate_weight).astype(jnp.bfloat16)
    signal = project(conv_input_weight).astype(jnp.bfloat16)
    conv_in = (inner_gate.astype(jnp.float32) * signal.astype(jnp.float32)).astype(jnp.bfloat16)
    padded = jnp.concatenate([jnp.zeros((TAPS - 1, CHANNELS), jnp.bfloat16), conv_in], axis=0)
    summed = jnp.zeros((TOKENS, CHANNELS), jnp.float32)
    for tap_index in range(TAPS):
        summed = summed + conv_taps[tap_index][None, :] * padded[tap_index:tap_index + TOKENS].astype(jnp.float32)
    conv_out = (outer_gate.astype(jnp.float32) * summed).astype(jnp.bfloat16)
    blocks = TOKENS // TOK_DEV

    def one_block(flat_index):
        head_index = flat_index // blocks
        row_start = (flat_index % blocks * TOK_DEV).astype(jnp.int32)
        query_rows = lax.dynamic_slice_in_dim(queries, row_start, TOK_DEV, 0)
        query_rows = lax.dynamic_index_in_dim(query_rows, head_index, 1, keepdims=False)
        head_keys = lax.dynamic_index_in_dim(key_rows, head_index, 1, keepdims=False)
        head_values = lax.dynamic_index_in_dim(values, head_index, 1, keepdims=False)
        scores = jnp.einsum('qcd,kcd->cqk', query_rows.astype(jnp.float32), head_keys.astype(jnp.float32)) * HEAD_DIM ** (-0.5)
        visible = (row_start + jnp.arange(TOK_DEV, dtype=jnp.int32))[:, None] >= jnp.arange(TOKENS, dtype=jnp.int32)[None, :]
        scores = jnp.where(visible[None], scores, MASKED)
        row_max = lax.optimization_barrier(jnp.max(scores, axis=-1, keepdims=True))
        exponent = jnp.where(visible[None], jnp.exp(scores - row_max), 0.0)
        row_sum = lax.optimization_barrier(jnp.sum(exponent, axis=-1, keepdims=True))
        normalized = exponent / row_sum
        lambda_value = lambdas[head_index]
        weights = (normalized[0] - lambda_value * normalized[1]).astype(jnp.bfloat16)
        head_mix = jnp.dot(weights, head_values, preferred_element_type=jnp.float32)
        normed = head_mix * lax.rsqrt(lax.optimization_barrier(jnp.mean(head_mix * head_mix, axis=-1, keepdims=True)) + HEAD_EPS) * head_gain[None, :] * HEAD_SCALE
        return (normed.astype(jnp.bfloat16), (row_max + jnp.log(row_sum))[..., 0])
    head_rows, log_rows = lax.map(one_block, jnp.arange(HEADS * blocks, dtype=jnp.int32))
    attn_out = jnp.transpose(head_rows.reshape(HEADS, blocks, TOK_DEV, 2 * HEAD_DIM), (1, 2, 0, 3)).reshape(TOKENS, CHANNELS)
    log_totals = jnp.transpose(log_rows.reshape(HEADS, blocks, 2, TOK_DEV), (0, 2, 1, 3)).reshape(HEADS, 2, TOKENS)
    mixed_out = jnp.dot(attn_out, attn_out_weight, preferred_element_type=jnp.float32) + jnp.dot(conv_out, conv_out_weight, preferred_element_type=jnp.float32)
    return (mixed_out.astype(jnp.bfloat16), log_totals)
```

```python
import math

import jax
import jax.numpy as jnp
from jax import lax
from jax.experimental import pallas as pl
from jax.experimental.pallas import tpu as pltpu
from jax.sharding import PartitionSpec as P

NORM_EPS = 1e-06
HEAD_EPS = 1e-05
ROPE_BASE = 500000.0
MASKED = -1e30
HEAD_SCALE = 0.8
MESH = pl.DeviceIdType.MESH

NY, NZ, NX, CORES = 4, 8, 4, 2
NTP = NX * CORES
ROWS = 512
HALF = ROWS // 2
PIECE = 256
DIM = 64
VDIM = 128
TILE = 256
LANES = 2 * TILE
TILES = NY * ROWS // TILE
ONES_ROWS = 16
LOG2E = math.log2(math.e)
LN2 = math.log(2.0)


def f32(x):
    return x.astype(jnp.float32)


def bf16(x):
    return x.astype(jnp.bfloat16)


def remote(src, dst, send_sem, recv_sem, device):
    return pltpu.make_async_remote_copy(
        src_ref=src,
        dst_ref=dst,
        send_sem=send_sem,
        recv_sem=recv_sem,
        device_id=device,
        device_id_type=MESH,
    )


class TpGather:
    def __init__(self, own, buf, send, recv, sp, x, c):
        self.own, self.buf, self.send, self.recv = own, buf, send, recv
        self.slot = lambda dx, other: lax.rem(x + dx + NX, NX) * CORES + (1 - c if other else c)
        self.partner = (sp, x * CORES + 1 - c)
        self.right = (sp, self.slot(1, False))
        self.left = (sp, self.slot(-1, False))
        self.started = 0

    def rows(self, h):
        half = self.buf.shape[1] // 2
        return pl.ds(h * half, half)

    def push(self, dx, h, device, first=False):
        slot = self.slot(dx, False)
        block = self.buf.at[slot, self.rows(h)]
        source = self.own.at[self.rows(h)] if first else block
        remote(source, block, self.send.at[self.started], self.recv.at[slot, h], device).start()
        self.started += 1

    def wait(self, dx, other, h):
        slot = self.slot(dx, other)
        block = self.buf.at[slot, self.rows(h)]
        remote(block, block, self.send.at[0], self.recv.at[slot, h], self.partner).wait_recv()

    def start(self):
        self.push(0, 0, self.right, True)
        self.push(0, 1, self.left, True)
        self.push(0, 1, self.right, True)
        self.push(0, 0, self.left, True)
        self.push(0, 0, self.partner, True)
        self.push(0, 1, self.partner, True)

    def neighbours_first(self):
        self.wait(-1, False, 0)
        self.push(-1, 0, self.right)
        self.push(-1, 0, self.partner)
        self.wait(1, False, 1)
        self.push(1, 1, self.left)
        self.push(1, 1, self.partner)

    def neighbours_second(self):
        self.wait(-1, False, 1)
        self.push(-1, 1, self.partner)
        self.wait(1, False, 0)
        self.push(1, 0, self.partner)

    def opposite(self, h):
        self.wait(2, False, h)
        self.push(2, h, self.partner)

    def finish(self):
        block = self.buf.at[0, self.rows(0)]
        for i in range(self.started):
            remote(block, block, self.send.at[i], self.recv.at[0, 0], self.partner).wait_send()


def kernel(
    tok, gain, wq, wk, wv, wo, wi, ws, cosine, sine, taps, lam, head_gain, wattn, wconv,
    out, logs,
    tbuf, wbuf, obuf, acc, ssq, kbuf, vbuf, qbuf, qbd, m_ref, a_ref, s_ref, stg, coef,
    csend, crecv, cown, ogate, cpad, tail_out, tail_in, convg, attng, oacc,
    w_sem, t_send, t_recv, ku_send, kd_send, vu_send, vd_send, k_recv, v_recv,
    q_send, q_recv, st_send, st_recv, c_send, c_recv, h_send, h_recv,
    g_send, g_recv, a_send, a_recv,
):
    sp, tp = lax.axis_index("sp"), lax.axis_index("tp")
    z, y = sp // NY, lax.rem(sp, NY)
    x, c = tp // CORES, lax.rem(tp, CORES)

    def at_y(step):
        return (z * NY + lax.rem(y + step, NY), tp)

    def at_z(step):
        return (lax.rem(z + step + NZ, NZ) * NY + y, tp)

    after = (lax.rem(sp + 1, NY * NZ), tp)
    before = (lax.rem(sp + NY * NZ - 1, NY * NZ), tp)

    tokens = TpGather(tok, tbuf, t_send, t_recv, sp, x, c)
    conv = TpGather(convg.at[tp], convg, g_send, g_recv, sp, x, c)
    attn = TpGather(attng.at[tp], attng, a_send, a_recv, sp, x, c)

    loads = [
        pltpu.make_async_copy(w, wbuf.at[:, :, i * VDIM : (i + 1) * VDIM], w_sem.at[i])
        for i, w in enumerate((wq, wk, wv, wo, wi, ws))
    ]
    loads += [
        pltpu.make_async_copy(w, obuf.at[i], w_sem.at[6 + i]) for i, w in enumerate((wattn, wconv))
    ]
    for load in loads:
        load.start()

    barrier = pltpu.get_barrier_semaphore()
    for device in (
        tokens.partner, tokens.left, tokens.right, at_y(1), at_y(2), at_y(3), at_z(1), at_z(-1), before,
    ):
        pl.semaphore_signal(barrier, inc=1, device_id=device, device_id_type=MESH)
    pl.semaphore_wait(barrier, 9)

    tokens.start()

    m_ref[...] = jnp.full_like(m_ref, MASKED)
    a_ref[...] = jnp.zeros_like(a_ref)
    qbd[...] = jnp.zeros_like(qbd)
    acc[...] = jnp.zeros_like(acc)
    ssq[...] = jnp.zeros_like(ssq)
    for load in loads[:6]:
        load.wait()

    def project(slot, h, src=None):
        rows = slice(h * HALF, (h + 1) * HALF)
        block = f32(tbuf[slot, rows] if src is None else src[rows])
        square = block * block
        ssq[rows] += square[:, :128] + square[:, 128:]
        scaled = bf16(block * gain[slot])
        acc[rows] += jnp.dot(scaled, wbuf[slot], preferred_element_type=jnp.float32)

    project(tp, 0, tok)
    project(tp, 1, tok)
    for h in (0, 1):
        tokens.wait(0, True, h)
        project(tokens.slot(0, True), h)
    tokens.neighbours_first()
    project(tokens.slot(-1, False), 0)
    project(tokens.slot(1, False), 1)
    tokens.neighbours_second()
    project(tokens.slot(-1, False), 1)
    project(tokens.slot(1, False), 0)
    for dx, h in ((-1, 0), (1, 1), (-1, 1), (1, 0)):
        tokens.wait(dx, True, h)
        project(tokens.slot(dx, True), h)
    for h in (0, 1):
        tokens.opposite(h)
        project(tokens.slot(2, False), h)
    for h in (0, 1):
        tokens.wait(2, True, h)
        project(tokens.slot(2, True), h)

    total = jnp.sum(ssq[...], axis=1, keepdims=True)
    inverse_rms = lax.rsqrt(total / (NTP * PIECE) + NORM_EPS)

    def projected(i):
        return inverse_rms * acc[:, i * VDIM : (i + 1) * VDIM]

    first_half = lax.rem(lax.broadcasted_iota(jnp.int32, (ROWS, VDIM), 1), DIM) < DIM // 2

    def turned(field):
        other = jnp.where(
            first_half, pltpu.roll(field, VDIM - DIM // 2, 1), pltpu.roll(field, DIM // 2, 1)
        )
        return field * cosine[...] + other * sine[...]

    kbuf[z] = bf16(turned(projected(1)))
    vbuf[z] = bf16(jnp.transpose(projected(2)))

    def k_copy(slot, send_sem, device):
        return remote(kbuf.at[slot], kbuf.at[slot], send_sem, k_recv.at[slot], device)

    def v_copy(slot, send_sem, device):
        return remote(vbuf.at[slot], vbuf.at[slot], send_sem, v_recv.at[slot], device)

    k_copy(z, ku_send.at[0], at_z(1)).start()
    k_copy(z, kd_send.at[0], at_z(-1)).start()
    v_copy(z, vu_send.at[0], at_z(1)).start()
    v_copy(z, vd_send.at[0], at_z(-1)).start()

    qbuf[y] = bf16(jnp.transpose(turned(projected(0))))
    q_copies = [
        remote(qbuf.at[y], qbuf.at[y], q_send.at[i - 1], q_recv.at[y], at_y(i)) for i in (1, 3, 2)
    ]
    for copy in q_copies:
        copy.start()

    ogate[...] = f32(bf16(projected(3)))
    conv_in = bf16(f32(bf16(projected(4))) * f32(bf16(projected(5))))
    cpad[8:] = f32(conv_in)
    tail_out[...] = conv_in[ROWS - 16 :]
    tail = remote(tail_out, tail_in, h_send, h_recv, after)
    tail.start()

    def blocked(block):
        scaled = f32(qbuf[block]) * (LOG2E * DIM**-0.5)
        high = bf16(scaled)
        low = bf16(scaled - f32(high))
        for h in (0, 1):
            lanes = slice(h * TILE, (h + 1) * TILE)
            for t, term in enumerate((high, low)):
                qbd[block * 2 + h, t * VDIM : t * VDIM + DIM, :TILE] = term[:DIM, lanes]
                qbd[block * 2 + h, t * VDIM + DIM : (t + 1) * VDIM, TILE:] = term[DIM:, lanes]

    ones = jnp.ones((ONES_ROWS, ROWS), jnp.bfloat16)

    def scores(slot, tile):
        keys = kbuf[slot]
        return jnp.dot(
            jnp.concatenate([keys, keys], axis=1), qbd[tile], preferred_element_type=jnp.float32
        )

    def absorb(slot, tile, s):
        m_old = m_ref[tile]
        m_new = jnp.maximum(m_old, jnp.max(s, axis=0, keepdims=True))
        keep = jnp.exp2(m_old - m_new)
        m_ref[tile] = m_new
        weights = bf16(jnp.exp2(s - m_new))
        a_ref[tile] = a_ref[tile] * keep + jnp.dot(
            jnp.concatenate([vbuf[slot], ones], axis=0), weights, preferred_element_type=jnp.float32
        )

    def whole_block(slot):
        s_ref[0] = scores(slot, 0)

        @pl.loop(0, TILES // 4)
        def _(g):
            for i in range(4):
                tile = g * 4 + i
                s_ref[(i + 1) % 2] = scores(slot, lax.rem(tile + 1, TILES))
                absorb(slot, tile, s_ref[i % 2])

    blocked(y)
    key_pos = lax.broadcasted_iota(jnp.int32, (ROWS, LANES), 0)
    query_pos = lax.rem(lax.broadcasted_iota(jnp.int32, (ROWS, LANES), 1), TILE)

    @pl.loop(0, 2)
    def _(h):
        s = jnp.where(key_pos <= query_pos + h * TILE, scores(z, y * 2 + h), MASKED)
        absorb(z, y * 2 + h, s)

    for i in (1, 3, 2):
        block = lax.rem(y + i, NY)
        remote(qbuf.at[block], qbuf.at[block], q_send.at[0], q_recv.at[block], at_y(1)).wait_recv()
        blocked(block)

    @pl.loop((y + 1) * 2, TILES)
    def _(tile):
        absorb(z, tile, scores(z, tile))

    tail.wait_recv()
    rim = f32(tail_in[8:])
    cpad[:8] = jnp.where(sp > 0, rim, jnp.zeros_like(rim))
    summed = taps[0:1] * cpad[6 : 6 + ROWS]
    summed += taps[1:2] * cpad[7 : 7 + ROWS]
    summed += taps[2:3] * cpad[8 : 8 + ROWS]
    convg[tp] = bf16(ogate[...] * summed)
    conv.start()

    @pl.loop(1, NZ // 2 + 1)
    def _(d):
        below, above = lax.rem(z - d + NZ, NZ), lax.rem(z + d, NZ)
        last = NZ // 2
        k_copy(below, ku_send.at[0], at_z(1)).wait_recv()

        @pl.when(d < last)
        def _():
            k_copy(below, ku_send.at[d], at_z(1)).start()
            k_copy(above, ku_send.at[0], at_z(1)).wait_recv()

        @pl.when(d < last - 1)
        def _():
            k_copy(above, kd_send.at[d], at_z(-1)).start()

        v_copy(above, vu_send.at[0], at_z(1)).wait_recv()

        @pl.when(d < last)
        def _():
            v_copy(above, vd_send.at[d], at_z(-1)).start()
            v_copy(below, vu_send.at[0], at_z(1)).wait_recv()

        @pl.when(d < last - 1)
        def _():
            v_copy(below, vu_send.at[d], at_z(1)).start()

        @pl.loop(0, 2)
        def _(r):
            source = jnp.where(r == 0, below, above)

            @pl.when((source < z) & ((d < last) | (r == 0)))
            def _():
                whole_block(source)

        @pl.when(d == 1)
        def _():
            conv.neighbours_first()
            conv.neighbours_second()

        @pl.when(d == 2)
        def _():
            conv.opposite(0)
            conv.opposite(1)

    for tile in range(TILES):
        stg[y, 0, tile : tile + 1] = m_ref[tile]
        stg[y, 1, tile : tile + 1] = a_ref[tile, VDIM : VDIM + 1]
    st_copies = [
        remote(stg.at[y], stg.at[y], st_send.at[i - 1], st_recv.at[y], at_y(i)) for i in (1, 3, 2)
    ]
    for copy in st_copies:
        copy.start()

    for load in loads[6:]:
        load.wait()
    for dx, h in ((-1, 0), (1, 1), (-1, 1), (1, 0), (0, 0), (0, 1), (2, 0), (2, 1)):
        conv.wait(dx, True, h)

    def mixed(buf, which, slot, rows):
        return jnp.dot(buf[slot, rows], obuf[which, slot], preferred_element_type=jnp.float32)

    oacc[...] = jnp.zeros_like(oacc)

    @pl.loop(0, NTP)
    def _(slot):
        oacc[...] += mixed(convg, 1, slot, slice(0, ROWS))

    for i in (1, 3, 2):
        peer = lax.rem(y + i, NY)
        remote(stg.at[peer], stg.at[peer], st_send.at[0], st_recv.at[peer], at_y(1)).wait_recv()
    m_all = stg[0, 0]
    for i in range(1, NY):
        m_all = jnp.maximum(m_all, stg[i, 0])
    l_all = stg[0, 1] * jnp.exp2(stg[0, 0] - m_all)
    for i in range(1, NY):
        l_all = l_all + stg[i, 1] * jnp.exp2(stg[i, 0] - m_all)
    second = lax.broadcasted_iota(jnp.int32, (TILES, LANES), 1) >= TILE
    share = jnp.exp2(stg[y, 0] - m_all) / l_all
    coef[0] = jnp.where(second, -lam[...] * share, share)
    coef[1] = m_all * LN2 + jnp.log(l_all)

    def combined(tile):
        part = a_ref[tile, :VDIM] * coef[0, pl.ds(tile, 1)]
        return part[:, :TILE] + part[:, TILE:]

    c_copies = []
    for i in (1, 3, 2):
        block = lax.rem(y + i, NY)
        for h in (0, 1):
            csend[block, :, h * TILE : (h + 1) * TILE] = bf16(combined(block * 2 + h))
        copy = remote(csend.at[block], crecv.at[y], c_send.at[i - 1], c_recv.at[y], at_y(i))
        copy.start()
        c_copies.append(copy)
    for h in (0, 1):
        lanes = slice(h * TILE, (h + 1) * TILE)
        cown[:, lanes] = combined(y * 2 + h)
        row = coef[1, pl.ds(y * 2 + h, 1)]
        logs[0:1, lanes] = row[:, :TILE]
        logs[1:2, lanes] = row[:, TILE:]
    for i in (1, 3, 2):
        peer = lax.rem(y + i, NY)
        remote(csend.at[peer], crecv.at[peer], c_send.at[0], c_recv.at[peer], at_y(1)).wait_recv()
        cown[...] += f32(crecv[peer])

    head_mix = cown[...]
    mean = jnp.sum(head_mix * head_mix, axis=0, keepdims=True) / VDIM
    normed = jnp.transpose(head_mix * lax.rsqrt(mean + HEAD_EPS))
    attng[tp] = bf16(normed * head_gain[...] * HEAD_SCALE)
    attn.start()

    def add(slot, h):
        rows = slice(h * HALF, (h + 1) * HALF)
        oacc[rows] += mixed(attng, 0, slot, rows)

    add(tp, 0)
    add(tp, 1)
    for h in (0, 1):
        attn.wait(0, True, h)
        add(attn.slot(0, True), h)
    attn.neighbours_first()
    add(attn.slot(-1, False), 0)
    add(attn.slot(1, False), 1)
    attn.neighbours_second()
    add(attn.slot(-1, False), 1)
    add(attn.slot(1, False), 0)
    for dx, h in ((-1, 0), (1, 1), (-1, 1), (1, 0)):
        attn.wait(dx, True, h)
        add(attn.slot(dx, True), h)
    for h in (0, 1):
        attn.opposite(h)
        add(attn.slot(2, False), h)
    for h in (0, 1):
        attn.wait(2, True, h)
        add(attn.slot(2, True), h)
    out[...] = bf16(oacc[...])

    tokens.finish()
    for d in range(NZ // 2):
        k_copy(z, ku_send.at[d], at_z(1)).wait_send()
        v_copy(z, vd_send.at[d], at_z(-1)).wait_send()
        if d < NZ // 2 - 1:
            k_copy(z, kd_send.at[d], at_z(-1)).wait_send()
            v_copy(z, vu_send.at[d], at_z(1)).wait_send()
    for copy in q_copies + st_copies + c_copies + [tail]:
        copy.wait_send()
    conv.finish()
    attn.finish()


def per_device(
    tokens,
    norm_gain,
    query_weight,
    key_weight,
    value_weight,
    outer_gate_weight,
    inner_gate_weight,
    conv_input_weight,
    conv_taps,
    lambdas,
    head_gain,
    attn_out_weight,
    conv_out_weight,
):
    half = DIM // 2
    frequency = ROPE_BASE ** (-jnp.arange(half, dtype=jnp.float32) * 2.0 / DIM)
    position = lax.axis_index("sp") * ROWS + jnp.arange(ROWS, dtype=jnp.int32)
    angles = position.astype(jnp.float32)[:, None] * frequency[None, :]
    cosine, sine = jnp.cos(angles), jnp.sin(angles)
    cosine = jnp.concatenate([cosine] * 4, axis=1)
    sine = jnp.concatenate([-sine, sine] * 2, axis=1)

    def in_pieces(weight):
        return weight.reshape(NTP, PIECE, VDIM)

    vmem = pl.BlockSpec(memory_space=pltpu.VMEM)
    anywhere = pl.BlockSpec(memory_space=pl.ANY)
    dma = pltpu.SemaphoreType.DMA
    bf, fl = jnp.bfloat16, jnp.float32
    mixed_out, logs = pl.pallas_call(
        kernel,
        out_shape=(
            jax.ShapeDtypeStruct((ROWS, PIECE), bf),
            jax.ShapeDtypeStruct((2, ROWS), fl),
        ),
        in_specs=[vmem, vmem] + [anywhere] * 6 + [vmem] * 5 + [anywhere] * 2,
        out_specs=(vmem, vmem),
        scratch_shapes=[
            pltpu.VMEM((NTP, ROWS, PIECE), bf),
            pltpu.VMEM((NTP, PIECE, 6 * VDIM), bf),
            pltpu.VMEM((2, NTP, VDIM, PIECE), bf),
            pltpu.VMEM((ROWS, 6 * VDIM), fl),
            pltpu.VMEM((ROWS, 128), fl),
            pltpu.VMEM((NZ, ROWS, VDIM), bf),
            pltpu.VMEM((NZ, VDIM, ROWS), bf),
            pltpu.VMEM((NY, VDIM, ROWS), bf),
            pltpu.VMEM((TILES, 2 * VDIM, LANES), bf),
            pltpu.VMEM((TILES, 1, LANES), fl),
            pltpu.VMEM((TILES, VDIM + ONES_ROWS, LANES), fl),
            pltpu.VMEM((2, ROWS, LANES), fl),
            pltpu.VMEM((NY, 2, TILES, LANES), fl),
            pltpu.VMEM((2, TILES, LANES), fl),
            pltpu.VMEM((NY, VDIM, ROWS), bf),
            pltpu.VMEM((NY, VDIM, ROWS), bf),
            pltpu.VMEM((VDIM, ROWS), fl),
            pltpu.VMEM((ROWS, VDIM), fl),
            pltpu.VMEM((8 + ROWS, VDIM), fl),
            pltpu.VMEM((16, VDIM), bf),
            pltpu.VMEM((16, VDIM), bf),
            pltpu.VMEM((NTP, ROWS, VDIM), bf),
            pltpu.VMEM((NTP, ROWS, VDIM), bf),
            pltpu.VMEM((ROWS, PIECE), fl),
            dma((8,)),
            dma((14,)),
            dma((NTP, 2)),
            dma((NZ // 2,)),
            dma((NZ // 2,)),
            dma((NZ // 2,)),
            dma((NZ // 2,)),
            dma((NZ,)),
            dma((NZ,)),
            dma((NY,)),
            dma((NY,)),
            dma((NY,)),
            dma((NY,)),
            dma((NY,)),
            dma((NY,)),
            dma,
            dma,
            dma((14,)),
            dma((NTP, 2)),
            dma((14,)),
            dma((NTP, 2)),
        ],
        compiler_params=pltpu.CompilerParams(
            collective_id=0, has_side_effects=True, vmem_limit_bytes=60 * 2**20
        ),
    )(
        tokens,
        norm_gain.reshape(NTP, 1, PIECE),
        *(
            in_pieces(w)
            for w in (
                query_weight,
                key_weight,
                value_weight,
                outer_gate_weight,
                inner_gate_weight,
                conv_input_weight,
            )
        ),
        cosine,
        sine,
        conv_taps,
        lambdas.reshape(1, 1),
        head_gain.reshape(1, VDIM),
        attn_out_weight.reshape(NTP, VDIM, PIECE),
        conv_out_weight.reshape(NTP, VDIM, PIECE),
    )
    return mixed_out, logs[None]


def solution(mesh):
    in_specs = (
        P("sp", "tp"),
        P(),
        P(None, "tp"),
        P(None, "tp"),
        P(None, "tp"),
        P(None, "tp"),
        P(None, "tp"),
        P(None, "tp"),
        P(None, "tp"),
        P("tp"),
        P(),
        P(None, "tp"),
        P(None, "tp"),
    )
    out_specs = (P("sp", "tp"), P("tp", None, "sp"))
    return jax.shard_map(
        per_device, mesh=mesh, in_specs=in_specs, out_specs=out_specs, check_vma=False
    )
```

```python
import math

import jax
import jax.numpy as jnp
import numpy as np
from jax import lax
from jax.experimental import pallas as pl
from jax.experimental.pallas import tpu as pltpu
from jax.sharding import PartitionSpec as P

NORM_EPS = 1e-06
HEAD_EPS = 1e-05
ROPE_BASE = 500000.0
MASKED = -1e30
HEAD_SCALE = 0.8
MESH = pl.DeviceIdType.MESH

NY, NZ, NX, CORES = 4, 8, 4, 2
NTP = NX * CORES
ROWS = 512
HALF = ROWS // 2
PIECE = 256
DIM = 64
VDIM = 128
TILE = 256
LANES = 2 * TILE
TILES = NY * ROWS // TILE
ONES_ROWS = 16
LOG2E = math.log2(math.e)
LN2 = math.log(2.0)


def f32(x):
    return x.astype(jnp.float32)


def bf16(x):
    return x.astype(jnp.bfloat16)


def remote(src, dst, send_sem, recv_sem, device):
    return pltpu.make_async_remote_copy(
        src_ref=src,
        dst_ref=dst,
        send_sem=send_sem,
        recv_sem=recv_sem,
        device_id=device,
        device_id_type=MESH,
    )


class TpGather:
    def __init__(self, own, buf, send, recv, sp, x, c):
        self.own, self.buf, self.send, self.recv = own, buf, send, recv
        self.slot = lambda dx, other: lax.rem(x + dx + NX, NX) * CORES + (1 - c if other else c)
        self.partner = (sp, x * CORES + 1 - c)
        self.right = (sp, self.slot(1, False))
        self.left = (sp, self.slot(-1, False))
        self.started = 0

    def rows(self, h):
        half = self.buf.shape[1] // 2
        return pl.ds(h * half, half)

    def push(self, dx, h, device, first=False):
        slot = self.slot(dx, False)
        block = self.buf.at[slot, self.rows(h)]
        source = self.own.at[self.rows(h)] if first else block
        remote(source, block, self.send.at[self.started], self.recv.at[slot, h], device).start()
        self.started += 1

    def wait(self, dx, other, h):
        slot = self.slot(dx, other)
        block = self.buf.at[slot, self.rows(h)]
        remote(block, block, self.send.at[0], self.recv.at[slot, h], self.partner).wait_recv()

    def start(self):
        self.push(0, 0, self.right, True)
        self.push(0, 1, self.left, True)
        self.push(0, 1, self.right, True)
        self.push(0, 0, self.left, True)
        self.push(0, 0, self.partner, True)
        self.push(0, 1, self.partner, True)

    def neighbours_first(self):
        self.wait(-1, False, 0)
        self.push(-1, 0, self.right)
        self.push(-1, 0, self.partner)
        self.wait(1, False, 1)
        self.push(1, 1, self.left)
        self.push(1, 1, self.partner)

    def neighbours_second(self):
        self.wait(-1, False, 1)
        self.push(-1, 1, self.partner)
        self.wait(1, False, 0)
        self.push(1, 0, self.partner)

    def opposite(self, h):
        self.wait(2, False, h)
        self.push(2, h, self.partner)

    def finish(self):
        block = self.buf.at[0, self.rows(0)]
        for i in range(self.started):
            remote(block, block, self.send.at[i], self.recv.at[0, 0], self.partner).wait_send()


def kernel(
    tok_in, gain_in, wq, wk, wv, wo, wi, ws, base_in, rows_in, taps_in, lam_in, head_gain_in,
    wattn, wconv,
    out, logs,
    tok, gain, base, turn, taps, lam, head_gain, tbuf, wbuf, obuf, acc, ssq, kbuf, vbuf, qbuf, qbd, m_ref, a_ref, s_ref, stg, coef,
    csend, crelay, crecv, cown, ogate, cpad, tail_out, tail_in, convg, attng, oacc,
    w_sem, i_sem, t_send, t_recv, ku_send, kd_send, vu_send, vd_send, k_recv, v_recv,
    q_send, q_recv, st_send, st_recv, c_send, c_recv, h_send, h_recv,
    g_send, g_recv, a_send, a_recv,
):
    sp, tp = lax.axis_index("sp"), lax.axis_index("tp")
    z, y = sp // NY, lax.rem(sp, NY)
    x, c = tp // CORES, lax.rem(tp, CORES)

    def at_y(step):
        return (z * NY + lax.rem(y + step, NY), tp)

    def at_z(step):
        return (lax.rem(z + step + NZ, NZ) * NY + y, tp)

    after = (lax.rem(sp + 1, NY * NZ), tp)
    before = (lax.rem(sp + NY * NZ - 1, NY * NZ), tp)

    tokens = TpGather(tok, tbuf, t_send, t_recv, sp, x, c)
    conv = TpGather(convg.at[tp], convg, g_send, g_recv, sp, x, c)
    attn = TpGather(attng.at[tp], attng, a_send, a_recv, sp, x, c)

    barrier = pltpu.get_barrier_semaphore()
    for device in (
        tokens.partner, tokens.left, tokens.right, at_y(1), at_y(2), at_y(3), at_z(1), at_z(-1), before,
    ):
        pl.semaphore_signal(barrier, inc=1, device_id=device, device_id_type=MESH)

    inputs = [
        pltpu.make_async_copy(source, target, i_sem.at[i])
        for i, (source, target) in enumerate(
            (
                (tok_in, tok),
                (gain_in, gain),
                (base_in.at[sp], base),
                (rows_in, turn),
                (taps_in, taps),
                (lam_in, lam),
                (head_gain_in, head_gain),
            )
        )
    ]
    loads = [
        pltpu.make_async_copy(w, wbuf.at[:, :, i * VDIM : (i + 1) * VDIM], w_sem.at[i])
        for i, w in enumerate((wq, wk, wv, wo, wi, ws))
    ]
    loads += [
        pltpu.make_async_copy(w, obuf.at[i], w_sem.at[6 + i]) for i, w in enumerate((wattn, wconv))
    ]
    for load in inputs + loads:
        load.start()
    inputs[0].wait()
    pl.semaphore_wait(barrier, 9)

    tokens.start()

    m_ref[...] = jnp.full_like(m_ref, MASKED)
    a_ref[...] = jnp.zeros_like(a_ref)
    qbd[...] = jnp.zeros_like(qbd)
    acc[...] = jnp.zeros_like(acc)
    ssq[...] = jnp.zeros_like(ssq)
    for load in inputs[1:] + loads[:6]:
        load.wait()

    block_cos, block_sin, signed_cos, signed_sin = (base[i : i + 1] for i in range(4))
    row_cos, row_sin = turn[0], turn[1]
    turn[0] = block_cos * row_cos - block_sin * row_sin
    turn[1] = signed_sin * row_cos + signed_cos * row_sin

    def project(slot, h, src=None):
        rows = slice(h * HALF, (h + 1) * HALF)
        block = f32(tbuf[slot, rows] if src is None else src[rows])
        square = block * block
        ssq[rows] += square[:, :128] + square[:, 128:]
        scaled = bf16(block * gain[slot])
        acc[rows] += jnp.dot(scaled, wbuf[slot], preferred_element_type=jnp.float32)

    project(tp, 0, tok)
    project(tp, 1, tok)
    for h in (0, 1):
        tokens.wait(0, True, h)
        project(tokens.slot(0, True), h)
    tokens.neighbours_first()
    project(tokens.slot(-1, False), 0)
    project(tokens.slot(1, False), 1)
    tokens.neighbours_second()
    project(tokens.slot(-1, False), 1)
    project(tokens.slot(1, False), 0)
    for dx, h in ((-1, 0), (1, 1), (-1, 1), (1, 0)):
        tokens.wait(dx, True, h)
        project(tokens.slot(dx, True), h)
    for h in (0, 1):
        tokens.opposite(h)
        project(tokens.slot(2, False), h)
    for h in (0, 1):
        tokens.wait(2, True, h)
        project(tokens.slot(2, True), h)

    total = jnp.sum(ssq[...], axis=1, keepdims=True)
    inverse_rms = lax.rsqrt(total / (NTP * PIECE) + NORM_EPS)

    def projected(i):
        return inverse_rms * acc[:, i * VDIM : (i + 1) * VDIM]

    first_half = lax.rem(lax.broadcasted_iota(jnp.int32, (ROWS, VDIM), 1), DIM) < DIM // 2

    def turned(field):
        other = jnp.where(
            first_half, pltpu.roll(field, VDIM - DIM // 2, 1), pltpu.roll(field, DIM // 2, 1)
        )
        return field * turn[0] + other * turn[1]

    kbuf[z] = bf16(turned(projected(1)))
    vbuf[z] = bf16(jnp.transpose(projected(2)))

    def k_copy(slot, send_sem, device):
        return remote(kbuf.at[slot], kbuf.at[slot], send_sem, k_recv.at[slot], device)

    def v_copy(slot, send_sem, device):
        return remote(vbuf.at[slot], vbuf.at[slot], send_sem, v_recv.at[slot], device)

    k_copy(z, ku_send.at[0], at_z(1)).start()
    k_copy(z, kd_send.at[0], at_z(-1)).start()
    v_copy(z, vu_send.at[0], at_z(1)).start()
    v_copy(z, vd_send.at[0], at_z(-1)).start()

    qbuf[y] = bf16(jnp.transpose(turned(projected(0))))
    q_copies = [
        remote(qbuf.at[y], qbuf.at[y], q_send.at[i - 1], q_recv.at[y], at_y(i)) for i in (1, 3, 2)
    ]
    for copy in q_copies:
        copy.start()

    ogate[...] = f32(bf16(projected(3)))
    conv_in = bf16(f32(bf16(projected(4))) * f32(bf16(projected(5))))
    cpad[8:] = f32(conv_in)
    tail_out[...] = conv_in[ROWS - 16 :]
    tail = remote(tail_out, tail_in, h_send, h_recv, after)
    tail.start()

    def blocked(block):
        scaled = f32(qbuf[block]) * (LOG2E * DIM**-0.5)
        high = bf16(scaled)
        low = bf16(scaled - f32(high))
        for h in (0, 1):
            lanes = slice(h * TILE, (h + 1) * TILE)
            for t, term in enumerate((high, low)):
                qbd[block * 2 + h, t * VDIM : t * VDIM + DIM, :TILE] = term[:DIM, lanes]
                qbd[block * 2 + h, t * VDIM + DIM : (t + 1) * VDIM, TILE:] = term[DIM:, lanes]

    ones = jnp.ones((ONES_ROWS, ROWS), jnp.bfloat16)

    def scores(slot, tile):
        keys = kbuf[slot]
        return jnp.dot(
            jnp.concatenate([keys, keys], axis=1), qbd[tile], preferred_element_type=jnp.float32
        )

    def absorb(slot, tile, s):
        m_old = m_ref[tile]
        m_new = jnp.maximum(m_old, jnp.max(s, axis=0, keepdims=True))
        keep = jnp.exp2(m_old - m_new)
        m_ref[tile] = m_new
        weights = bf16(jnp.exp2(s - m_new))
        a_ref[tile] = a_ref[tile] * keep + jnp.dot(
            jnp.concatenate([vbuf[slot], ones], axis=0), weights, preferred_element_type=jnp.float32
        )

    def whole_block(slot):
        s_ref[0] = scores(slot, 0)

        @pl.loop(0, TILES // 4)
        def _(g):
            for i in range(4):
                tile = g * 4 + i
                s_ref[(i + 1) % 2] = scores(slot, lax.rem(tile + 1, TILES))
                absorb(slot, tile, s_ref[i % 2])

    blocked(y)
    key_pos = lax.broadcasted_iota(jnp.int32, (ROWS, LANES), 0)
    query_pos = lax.rem(lax.broadcasted_iota(jnp.int32, (ROWS, LANES), 1), TILE)

    @pl.loop(0, 2)
    def _(h):
        s = jnp.where(key_pos <= query_pos + h * TILE, scores(z, y * 2 + h), MASKED)
        absorb(z, y * 2 + h, s)

    last = NZ // 2

    def pass_keys(d):
        below, above = lax.rem(z - d + NZ, NZ), lax.rem(z + d, NZ)
        k_copy(below, ku_send.at[0], at_z(1)).wait_recv()

        @pl.when(d < last)
        def _():
            k_copy(below, ku_send.at[d], at_z(1)).start()
            k_copy(above, ku_send.at[0], at_z(1)).wait_recv()

        @pl.when(d < last - 1)
        def _():
            k_copy(above, kd_send.at[d], at_z(-1)).start()

    def pass_values(d):
        below, above = lax.rem(z - d + NZ, NZ), lax.rem(z + d, NZ)
        v_copy(above, vu_send.at[0], at_z(1)).wait_recv()

        @pl.when(d < last)
        def _():
            v_copy(above, vd_send.at[d], at_z(-1)).start()
            v_copy(below, vu_send.at[0], at_z(1)).wait_recv()

        @pl.when(d < last - 1)
        def _():
            v_copy(below, vu_send.at[d], at_z(1)).start()

    for i in (1, 3, 2):
        block = lax.rem(y + i, NY)
        remote(qbuf.at[block], qbuf.at[block], q_send.at[0], q_recv.at[block], at_y(1)).wait_recv()
        blocked(block)
        if i == 3:
            pass_keys(1)

    tail.wait_recv()
    rim = f32(tail_in[8:])
    cpad[:8] = jnp.where(sp > 0, rim, jnp.zeros_like(rim))
    summed = taps[0:1] * cpad[6 : 6 + ROWS]
    summed += taps[1:2] * cpad[7 : 7 + ROWS]
    summed += taps[2:3] * cpad[8 : 8 + ROWS]
    convg[tp] = bf16(ogate[...] * summed)
    conv.start()

    @pl.loop(y + 1, NY)
    def _(block):
        for h in (0, 1):
            s_ref[h] = scores(z, block * 2 + h)
        for h in (0, 1):
            absorb(z, block * 2 + h, s_ref[h])

    pass_values(1)

    @pl.loop(0, NZ - 1)
    def _(i):
        d, r = i // 2 + 1, lax.rem(i, 2)
        source = lax.rem(z + jnp.where(r == 0, NZ - d, d), NZ)

        @pl.when(source < z)
        def _():
            whole_block(source)

        @pl.when((r == 0) & (d < last))
        def _():
            pass_keys(d + 1)

        @pl.when(r == 1)
        def _():
            pass_values(d + 1)

        @pl.when(i == 1)
        def _():
            conv.neighbours_first()
            conv.neighbours_second()

        @pl.when(i == 3)
        def _():
            conv.opposite(0)
            conv.opposite(1)

    for tile in range(TILES):
        stg[y, 0, tile : tile + 1] = m_ref[tile]
        stg[y, 1, tile : tile + 1] = a_ref[tile, VDIM : VDIM + 1]
    st_copies = [
        remote(stg.at[y], stg.at[y], st_send.at[i - 1], st_recv.at[y], at_y(i)) for i in (1, 3, 2)
    ]
    for copy in st_copies:
        copy.start()

    for load in loads[6:]:
        load.wait()
    for dx, h in ((-1, 0), (1, 1), (-1, 1), (1, 0), (0, 0), (0, 1), (2, 0), (2, 1)):
        conv.wait(dx, True, h)

    def mixed(buf, which, slot, rows):
        return jnp.dot(buf[slot, rows], obuf[which, slot], preferred_element_type=jnp.float32)

    oacc[...] = jnp.zeros_like(oacc)

    @pl.loop(0, NTP)
    def _(slot):
        oacc[...] += mixed(convg, 1, slot, slice(0, ROWS))

    for i in (1, 3, 2):
        peer = lax.rem(y + i, NY)
        remote(stg.at[peer], stg.at[peer], st_send.at[0], st_recv.at[peer], at_y(1)).wait_recv()
    m_all = stg[0, 0]
    for i in range(1, NY):
        m_all = jnp.maximum(m_all, stg[i, 0])
    l_all = stg[0, 1] * jnp.exp2(stg[0, 0] - m_all)
    for i in range(1, NY):
        l_all = l_all + stg[i, 1] * jnp.exp2(stg[i, 0] - m_all)
    second = lax.broadcasted_iota(jnp.int32, (TILES, LANES), 1) >= TILE
    share = jnp.exp2(stg[y, 0] - m_all) / l_all
    coef[0] = jnp.where(second, -lam[0:1, 0:1] * share, share)
    coef[1] = m_all * LN2 + jnp.log(l_all)

    def combined(tile):
        part = a_ref[tile, :VDIM] * coef[0, pl.ds(tile, 1)]
        return part[:, :TILE] + part[:, TILE:]

    right, left = lax.rem(y + 1, NY), lax.rem(y + 3, NY)
    opposite = lax.rem(y + 2, NY)
    to = (at_y(1), at_y(-1 + NY))
    near = (right, left)
    c_copies = []

    def send_part(i, target, device):
        copy = remote(csend.at[i], target, c_send.at[i], c_recv.at[i], device)
        copy.start()
        c_copies.append(copy)

    for w in (0, 1):
        csend[w] = bf16(combined(opposite * 2 + w))
    for w in (0, 1):
        send_part(w, crelay.at[w], to[w])
    for w in (0, 1):
        csend[2 + w] = bf16(combined(near[w] * 2 + 1 - w))
    for w in (0, 1):
        send_part(2 + w, crecv.at[w, 0], to[w])
    relayed = [combined(near[w] * 2 + w) for w in (0, 1)]
    for w in (0, 1):
        c_copies[w].wait_recv()
        csend[4 + w] = bf16(relayed[w] + f32(crelay[w]))
        send_part(4 + w, crecv.at[w, 1], to[w])
    for h in (0, 1):
        lanes = slice(h * TILE, (h + 1) * TILE)
        cown[:, lanes] = combined(y * 2 + h)
        row = coef[1, pl.ds(y * 2 + h, 1)]
        logs[0, 0:1, lanes] = row[:, :TILE]
        logs[0, 1:2, lanes] = row[:, TILE:]
    for w in (0, 1):
        c_copies[2 + w].wait_recv()
        cown[:, (1 - w) * TILE : (2 - w) * TILE] += f32(crecv[w, 0])
    for w in (0, 1):
        c_copies[4 + w].wait_recv()
        cown[:, w * TILE : (w + 1) * TILE] += f32(crecv[w, 1])

    head_mix = cown[...]
    mean = jnp.sum(head_mix * head_mix, axis=0, keepdims=True) / VDIM
    normed = jnp.transpose(head_mix * lax.rsqrt(mean + HEAD_EPS))
    attng[tp] = bf16(normed * head_gain[...] * HEAD_SCALE)
    attn.start()

    def add(slot, h):
        rows = slice(h * HALF, (h + 1) * HALF)
        oacc[rows] += mixed(attng, 0, slot, rows)

    add(tp, 0)
    add(tp, 1)
    for h in (0, 1):
        attn.wait(0, True, h)
        add(attn.slot(0, True), h)
    attn.neighbours_first()
    add(attn.slot(-1, False), 0)
    add(attn.slot(1, False), 1)
    attn.neighbours_second()
    add(attn.slot(-1, False), 1)
    add(attn.slot(1, False), 0)
    for dx, h in ((-1, 0), (1, 1), (-1, 1), (1, 0)):
        attn.wait(dx, True, h)
        add(attn.slot(dx, True), h)
    for h in (0, 1):
        attn.opposite(h)
        add(attn.slot(2, False), h)
    for h in (0, 1):
        attn.wait(2, True, h)
        add(attn.slot(2, True), h)
    out[...] = bf16(oacc[...])

    tokens.finish()
    for d in range(NZ // 2):
        k_copy(z, ku_send.at[d], at_z(1)).wait_send()
        v_copy(z, vd_send.at[d], at_z(-1)).wait_send()
        if d < NZ // 2 - 1:
            k_copy(z, kd_send.at[d], at_z(-1)).wait_send()
            v_copy(z, vu_send.at[d], at_z(1)).wait_send()
    for copy in q_copies + st_copies + c_copies + [tail]:
        copy.wait_send()
    conv.finish()
    attn.finish()


def per_device(
    tokens,
    norm_gain,
    query_weight,
    key_weight,
    value_weight,
    outer_gate_weight,
    inner_gate_weight,
    conv_input_weight,
    conv_taps,
    lambdas,
    head_gain,
    attn_out_weight,
    conv_out_weight,
):
    half = DIM // 2
    frequency = np.float32(ROPE_BASE) ** (-np.arange(half, dtype=np.float32) * 2.0 / DIM)
    frequency = np.tile(frequency.astype(np.float64), 4)
    sign = np.tile(np.repeat([-1.0, 1.0], half), 2)
    start = np.arange(NY * NZ)[:, None] * ROWS * frequency
    cosine, sine = np.cos(start), np.sin(start)
    base = np.stack([cosine, sine, sign * cosine, sign * sine], axis=1).astype(np.float32)
    row = np.arange(ROWS)[:, None] * frequency
    rows = np.stack([np.cos(row), np.sin(row)]).astype(np.float32)

    def in_pieces(weight):
        return weight.reshape(NTP, PIECE, VDIM)

    vmem = pl.BlockSpec(memory_space=pltpu.VMEM)
    anywhere = pl.BlockSpec(memory_space=pltpu.HBM)
    dma = pltpu.SemaphoreType.DMA
    bf, fl = jnp.bfloat16, jnp.float32
    mixed_out, logs = pl.pallas_call(
        kernel,
        out_shape=(
            jax.ShapeDtypeStruct((ROWS, PIECE), bf),
            jax.ShapeDtypeStruct((1, 2, ROWS), fl),
        ),
        in_specs=[anywhere] * 15,
        out_specs=(vmem, vmem),
        scratch_shapes=[
            pltpu.VMEM((ROWS, PIECE), bf),
            pltpu.VMEM((NTP, 1, PIECE), fl),
            pltpu.VMEM((4, 128), fl),
            pltpu.VMEM((2, ROWS, 128), fl),
            pltpu.VMEM((3, VDIM), fl),
            pltpu.VMEM((1, 128), fl),
            pltpu.VMEM((1, VDIM), fl),
            pltpu.VMEM((NTP, ROWS, PIECE), bf),
            pltpu.VMEM((NTP, PIECE, 6 * VDIM), bf),
            pltpu.VMEM((2, NTP, VDIM, PIECE), bf),
            pltpu.VMEM((ROWS, 6 * VDIM), fl),
            pltpu.VMEM((ROWS, 128), fl),
            pltpu.VMEM((NZ, ROWS, VDIM), bf),
            pltpu.VMEM((NZ, VDIM, ROWS), bf),
            pltpu.VMEM((NY, VDIM, ROWS), bf),
            pltpu.VMEM((TILES, 2 * VDIM, LANES), bf),
            pltpu.VMEM((TILES, 1, LANES), fl),
            pltpu.VMEM((TILES, VDIM + ONES_ROWS, LANES), fl),
            pltpu.VMEM((2, ROWS, LANES), fl),
            pltpu.VMEM((NY, 2, TILES, LANES), fl),
            pltpu.VMEM((2, TILES, LANES), fl),
            pltpu.VMEM((6, VDIM, TILE), bf),
            pltpu.VMEM((2, VDIM, TILE), bf),
            pltpu.VMEM((2, 2, VDIM, TILE), bf),
            pltpu.VMEM((VDIM, ROWS), fl),
            pltpu.VMEM((ROWS, VDIM), fl),
            pltpu.VMEM((8 + ROWS, VDIM), fl),
            pltpu.VMEM((16, VDIM), bf),
            pltpu.VMEM((16, VDIM), bf),
            pltpu.VMEM((NTP, ROWS, VDIM), bf),
            pltpu.VMEM((NTP, ROWS, VDIM), bf),
            pltpu.VMEM((ROWS, PIECE), fl),
            dma((8,)),
            dma((7,)),
            dma((14,)),
            dma((NTP, 2)),
            dma((NZ // 2,)),
            dma((NZ // 2,)),
            dma((NZ // 2,)),
            dma((NZ // 2,)),
            dma((NZ,)),
            dma((NZ,)),
            dma((NY,)),
            dma((NY,)),
            dma((NY,)),
            dma((NY,)),
            dma((6,)),
            dma((6,)),
            dma,
            dma,
            dma((14,)),
            dma((NTP, 2)),
            dma((14,)),
            dma((NTP, 2)),
        ],
        compiler_params=pltpu.CompilerParams(
            collective_id=0, has_side_effects=True, vmem_limit_bytes=60 * 2**20
        ),
    )(
        tokens,
        norm_gain.reshape(NTP, 1, PIECE),
        *(
            in_pieces(w)
            for w in (
                query_weight,
                key_weight,
                value_weight,
                outer_gate_weight,
                inner_gate_weight,
                conv_input_weight,
            )
        ),
        jnp.asarray(base),
        jnp.asarray(rows),
        conv_taps,
        jnp.broadcast_to(lambdas, (1, 128)),
        head_gain.reshape(1, VDIM),
        attn_out_weight.reshape(NTP, VDIM, PIECE),
        conv_out_weight.reshape(NTP, VDIM, PIECE),
    )
    return mixed_out, logs


def solution(mesh):
    in_specs = (
        P("sp", "tp"),
        P(),
        P(None, "tp"),
        P(None, "tp"),
        P(None, "tp"),
        P(None, "tp"),
        P(None, "tp"),
        P(None, "tp"),
        P(None, "tp"),
        P("tp"),
        P(),
        P(None, "tp"),
        P(None, "tp"),
    )
    out_specs = (P("sp", "tp"), P("tp", None, "sp"))
    return jax.shard_map(
        per_device, mesh=mesh, in_specs=in_specs, out_specs=out_specs, check_vma=False
    )
```

```python
import math

import jax
import jax.numpy as jnp
import numpy as np
from jax import lax
from jax.experimental import pallas as pl
from jax.experimental.pallas import tpu as pltpu
from jax.sharding import PartitionSpec as P

NORM_EPS = 1e-06
HEAD_EPS = 1e-05
ROPE_BASE = 500000.0
MASKED = -1e30
HEAD_SCALE = 0.8
MESH = pl.DeviceIdType.MESH

NY, NZ, NX, CORES = 4, 8, 4, 2
NTP = NX * CORES
ROWS = 512
HALF = ROWS // 2
PIECE = 256
DIM = 64
VDIM = 128
TILE = 256
LANES = 2 * TILE
TILES = NY * ROWS // TILE
ONES_ROWS = 16
LOG2E = math.log2(math.e)
LN2 = math.log(2.0)


def f32(x):
    return x.astype(jnp.float32)


def bf16(x):
    return x.astype(jnp.bfloat16)


def remote(src, dst, send_sem, recv_sem, device):
    return pltpu.make_async_remote_copy(
        src_ref=src,
        dst_ref=dst,
        send_sem=send_sem,
        recv_sem=recv_sem,
        device_id=device,
        device_id_type=MESH,
    )


class TpGather:
    def __init__(self, own, buf, send, recv, parts, sp, x, c):
        self.own, self.buf, self.send, self.recv, self.parts = own, buf, send, recv, parts
        self.slot = lambda dx, other: lax.rem(x + dx + NX, NX) * CORES + (1 - c if other else c)
        self.partner = (sp, x * CORES + 1 - c)
        self.right = (sp, self.slot(1, False))
        self.left = (sp, self.slot(-1, False))
        self.started = 0

    def rows(self, p):
        size = self.buf.shape[1] // self.parts
        return pl.ds(p * size, size)

    def push(self, dx, p, device, first=False):
        slot = self.slot(dx, False)
        block = self.buf.at[slot, self.rows(p)]
        source = self.own.at[self.rows(p)] if first else block
        remote(source, block, self.send.at[self.started], self.recv.at[slot, p], device).start()
        self.started += 1

    def wait(self, dx, other, *parts):
        slot = self.slot(dx, other)
        for p in parts:
            block = self.buf.at[slot, self.rows(p)]
            remote(block, block, self.send.at[0], self.recv.at[slot, p], self.partner).wait_recv()

    def start(self, *pairs):
        for p in pairs:
            self.push(0, p, self.right, True)
            self.push(0, p + 1, self.left, True)
        for p in pairs:
            self.push(0, p + 1, self.right, True)
            self.push(0, p, self.left, True)
        for p in pairs:
            self.push(0, p, self.partner, True)
            self.push(0, p + 1, self.partner, True)

    def neighbours_first(self, *pairs):
        for p in pairs:
            self.wait(-1, False, p)
            self.push(-1, p, self.right)
            self.wait(1, False, p + 1)
            self.push(1, p + 1, self.left)
        for p in pairs:
            self.push(-1, p, self.partner)
            self.push(1, p + 1, self.partner)

    def neighbours_second(self, *pairs):
        for p in pairs:
            self.wait(-1, False, p + 1)
            self.push(-1, p + 1, self.partner)
            self.wait(1, False, p)
            self.push(1, p, self.partner)

    def opposite(self, *parts):
        for p in parts:
            self.wait(2, False, p)
            self.push(2, p, self.partner)

    def finish(self):
        block = self.buf.at[0, self.rows(0)]
        for i in range(self.started):
            remote(block, block, self.send.at[i], self.recv.at[0, 0], self.partner).wait_send()


def kernel(
    tok_in, gain_in, wq, wk, wv, wo, wi, ws, base_in, rows_in, taps_in, lam_in, head_gain_in,
    wattn, wconv,
    out, logs,
    tok, gain, base, turn, taps, lam, head_gain, tbuf, wbuf, obuf, acc, ssq, kbuf, vbuf, qbuf, qbd, m_ref, a_ref, s_ref, stg, coef,
    csend, crelay, crecv, cown, ogate, cpad, tail_out, tail_in, convg, attng, oacc,
    w_sem, i_sem, t_send, t_recv, ku_send, kd_send, vu_send, vd_send, k_recv, v_recv,
    q_send, q_recv, st_send, st_recv, c_send, c_recv, h_send, h_recv,
    g_send, g_recv, a_send, a_recv,
):
    sp, tp = lax.axis_index("sp"), lax.axis_index("tp")
    z, y = sp // NY, lax.rem(sp, NY)
    x, c = tp // CORES, lax.rem(tp, CORES)

    def at_y(step):
        return (z * NY + lax.rem(y + step, NY), tp)

    def at_z(step):
        return (lax.rem(z + step + NZ, NZ) * NY + y, tp)

    after = (lax.rem(sp + 1, NY * NZ), tp)
    before = (lax.rem(sp + NY * NZ - 1, NY * NZ), tp)

    tokens = TpGather(tok, tbuf, t_send, t_recv, 2, sp, x, c)
    conv = TpGather(convg.at[tp], convg, g_send, g_recv, 2, sp, x, c)
    attn = TpGather(attng.at[tp], attng, a_send, a_recv, 4, sp, x, c)

    barrier = pltpu.get_barrier_semaphore()
    for device in (
        tokens.partner, tokens.left, tokens.right, at_y(1), at_y(2), at_y(3), at_z(1), at_z(-1), before,
    ):
        pl.semaphore_signal(barrier, inc=1, device_id=device, device_id_type=MESH)

    inputs = [
        pltpu.make_async_copy(source, target, i_sem.at[i])
        for i, (source, target) in enumerate(
            (
                (tok_in, tok),
                (gain_in, gain),
                (base_in.at[sp], base),
                (rows_in, turn),
                (taps_in, taps),
                (lam_in, lam),
                (head_gain_in, head_gain),
            )
        )
    ]
    loads = [
        pltpu.make_async_copy(w, wbuf.at[:, :, i * VDIM : (i + 1) * VDIM], w_sem.at[i])
        for i, w in enumerate((wq, wk, wv, wo, wi, ws))
    ]
    loads += [
        pltpu.make_async_copy(w, obuf.at[i], w_sem.at[6 + i]) for i, w in enumerate((wattn, wconv))
    ]
    for load in inputs + loads:
        load.start()
    inputs[0].wait()
    pl.semaphore_wait(barrier, 9)

    tokens.start(0)

    m_ref[...] = jnp.full_like(m_ref, MASKED)
    a_ref[...] = jnp.zeros_like(a_ref)
    qbd[...] = jnp.zeros_like(qbd)
    acc[...] = jnp.zeros_like(acc)
    ssq[...] = jnp.zeros_like(ssq)
    for load in inputs[1:] + loads[:6]:
        load.wait()

    block_cos, block_sin, signed_cos, signed_sin = (base[i : i + 1] for i in range(4))
    row_cos, row_sin = turn[0], turn[1]
    turn[0] = block_cos * row_cos - block_sin * row_sin
    turn[1] = signed_sin * row_cos + signed_cos * row_sin

    def project(slot, h, src=None):
        rows = slice(h * HALF, (h + 1) * HALF)
        block = f32(tbuf[slot, rows] if src is None else src[rows])
        square = block * block
        ssq[rows] += square[:, :128] + square[:, 128:]
        scaled = bf16(block * gain[slot])
        acc[rows] += jnp.dot(scaled, wbuf[slot], preferred_element_type=jnp.float32)

    def gathered(gather, use):
        each = gather.parts // 2
        halves = (range(each), range(each, 2 * each))
        pairs = range(0, gather.parts, 2)
        for h in (0, 1):
            gather.wait(0, True, *halves[h])
            use(gather.slot(0, True), h)
        gather.neighbours_first(*pairs)
        gather.neighbours_second(*pairs)
        for dx in (-1, 1):
            for h in (0, 1):
                use(gather.slot(dx, False), h)
        for dx in (-1, 1):
            for h in (0, 1):
                gather.wait(dx, True, *halves[h])
                use(gather.slot(dx, True), h)
        gather.opposite(*halves[0], *halves[1])
        for other in (False, True):
            for h in (0, 1):
                if other:
                    gather.wait(2, True, *halves[h])
                use(gather.slot(2, other), h)

    project(tp, 0, tok)
    project(tp, 1, tok)
    gathered(tokens, project)

    total = jnp.sum(ssq[...], axis=1, keepdims=True)
    inverse_rms = lax.rsqrt(total / (NTP * PIECE) + NORM_EPS)

    def projected(i):
        return inverse_rms * acc[:, i * VDIM : (i + 1) * VDIM]

    first_half = lax.rem(lax.broadcasted_iota(jnp.int32, (ROWS, VDIM), 1), DIM) < DIM // 2

    def turned(field):
        other = jnp.where(
            first_half, pltpu.roll(field, VDIM - DIM // 2, 1), pltpu.roll(field, DIM // 2, 1)
        )
        return field * turn[0] + other * turn[1]

    kbuf[z] = bf16(turned(projected(1)))
    vbuf[z] = bf16(jnp.transpose(projected(2)))

    def k_copy(slot, send_sem, device):
        return remote(kbuf.at[slot], kbuf.at[slot], send_sem, k_recv.at[slot], device)

    def v_copy(slot, send_sem, device):
        return remote(vbuf.at[slot], vbuf.at[slot], send_sem, v_recv.at[slot], device)

    k_copy(z, ku_send.at[0], at_z(1)).start()
    k_copy(z, kd_send.at[0], at_z(-1)).start()
    v_copy(z, vu_send.at[0], at_z(1)).start()
    v_copy(z, vd_send.at[0], at_z(-1)).start()

    qbuf[y] = bf16(jnp.transpose(turned(projected(0))))
    q_copies = [
        remote(qbuf.at[y], qbuf.at[y], q_send.at[i - 1], q_recv.at[y], at_y(i)) for i in (1, 3, 2)
    ]
    for copy in q_copies:
        copy.start()

    ogate[...] = f32(bf16(projected(3)))
    conv_in = bf16(f32(bf16(projected(4))) * f32(bf16(projected(5))))
    cpad[8:] = f32(conv_in)
    tail_out[...] = conv_in[ROWS - 16 :]
    tail = remote(tail_out, tail_in, h_send, h_recv, after)
    tail.start()

    def blocked(block):
        scaled = f32(qbuf[block]) * (LOG2E * DIM**-0.5)
        high = bf16(scaled)
        low = bf16(scaled - f32(high))
        for h in (0, 1):
            lanes = slice(h * TILE, (h + 1) * TILE)
            for t, term in enumerate((high, low)):
                qbd[h * NY + block, t * VDIM : t * VDIM + DIM, :TILE] = term[:DIM, lanes]
                qbd[h * NY + block, t * VDIM + DIM : (t + 1) * VDIM, TILE:] = term[DIM:, lanes]

    ones = jnp.ones((ONES_ROWS, ROWS), jnp.bfloat16)

    def scores(slot, tile, count=ROWS):
        keys = kbuf[slot, :count]
        return jnp.dot(
            jnp.concatenate([keys, keys], axis=1), qbd[tile], preferred_element_type=jnp.float32
        )

    def absorb(slot, tile, s, count=ROWS):
        m_old = m_ref[tile]
        m_new = jnp.maximum(m_old, jnp.max(s, axis=0, keepdims=True))
        keep = jnp.exp2(m_old - m_new)
        m_ref[tile] = m_new
        weights = bf16(jnp.exp2(s - m_new))
        a_ref[tile] = a_ref[tile] * keep + jnp.dot(
            jnp.concatenate([vbuf[slot, :, :count], ones[:, :count]], axis=0),
            weights,
            preferred_element_type=jnp.float32,
        )

    def four_tiles(slot, g):
        for i in range(4):
            tile = g * 4 + i
            s_ref[(i + 1) % 2] = scores(slot, lax.rem(tile + 1, TILES))
            absorb(slot, tile, s_ref[i % 2])

    blocked(y)
    for h in (0, 1):
        count = (h + 1) * TILE
        key_pos = lax.broadcasted_iota(jnp.int32, (count, LANES), 0)
        query_pos = lax.rem(lax.broadcasted_iota(jnp.int32, (count, LANES), 1), TILE) + h * TILE
        s = jnp.where(key_pos <= query_pos, scores(z, h * NY + y, count), MASKED)
        absorb(z, h * NY + y, s, count)

    last = NZ // 2

    def pass_keys(d):
        below, above = lax.rem(z - d + NZ, NZ), lax.rem(z + d, NZ)
        k_copy(below, ku_send.at[0], at_z(1)).wait_recv()

        @pl.when(d < last)
        def _():
            k_copy(below, ku_send.at[d], at_z(1)).start()
            k_copy(above, ku_send.at[0], at_z(1)).wait_recv()

        @pl.when(d < last - 1)
        def _():
            k_copy(above, kd_send.at[d], at_z(-1)).start()

    def pass_values(d):
        below, above = lax.rem(z - d + NZ, NZ), lax.rem(z + d, NZ)
        v_copy(above, vu_send.at[0], at_z(1)).wait_recv()

        @pl.when(d < last)
        def _():
            v_copy(above, vd_send.at[d], at_z(-1)).start()
            v_copy(below, vu_send.at[0], at_z(1)).wait_recv()

        @pl.when(d < last - 1)
        def _():
            v_copy(below, vu_send.at[d], at_z(1)).start()

    pass_keys(1)

    for i in (1, 3, 2):
        block = lax.rem(y + i, NY)
        remote(qbuf.at[block], qbuf.at[block], q_send.at[0], q_recv.at[block], at_y(1)).wait_recv()
        blocked(block)

    @pl.when(y < NY - 1)
    def _():
        s_ref[0] = scores(z, y + 1)

        @pl.loop(y + 1, NY)
        def _(block):
            s_ref[1] = scores(z, NY + block)
            absorb(z, block, s_ref[0])
            s_ref[0] = scores(z, lax.rem(block + 1, NY))
            absorb(z, NY + block, s_ref[1])

    pass_values(1)

    tail.wait_recv()
    rim = f32(tail_in[8:])
    cpad[:8] = jnp.where(sp > 0, rim, jnp.zeros_like(rim))
    summed = taps[0:1] * cpad[6 : 6 + ROWS]
    summed += taps[1:2] * cpad[7 : 7 + ROWS]
    summed += taps[2:3] * cpad[8 : 8 + ROWS]
    convg[tp] = bf16(ogate[...] * summed)
    conv.start(0)

    def half_block(source, g):
        @pl.when((source < z) & (g == 0))
        def _():
            s_ref[0] = scores(source, 0)

        @pl.when(source < z)
        def _():
            four_tiles(source, g)

    @pl.loop(0, NZ - 2)
    def _(i):
        d, r = i // 2 + 1, lax.rem(i, 2)
        source = lax.rem(z + jnp.where(r == 0, NZ - d, d), NZ)

        @pl.loop(0, 2)
        def _(g):
            @pl.when((g == 1) & (r == 0))
            def _():
                pass_keys(d + 1)

            @pl.when((g == 1) & (r == 1))
            def _():
                pass_values(d + 1)

            half_block(source, g)

        @pl.when(i == 1)
        def _():
            conv.neighbours_first(0)
            conv.neighbours_second(0)

        @pl.when(i == 3)
        def _():
            conv.opposite(0, 1)

    def st_copy(h, i):
        return remote(stg.at[y, h], stg.at[y, h], st_send.at[h, i - 1], st_recv.at[y, h], at_y(i))

    @pl.loop(0, 2)
    def _(h):
        half_block(lax.rem(z + last, NZ), h)
        for t in range(NY):
            stg[y, h, t : t + 1] = m_ref[h * NY + t]
            stg[y, h, NY + t : NY + t + 1] = a_ref[h * NY + t, VDIM : VDIM + 1]
        for i in (2, 1, 3):
            st_copy(h, i).start()

    for load in loads[6:]:
        load.wait()
    for dx, h in ((-1, 0), (1, 1), (-1, 1), (1, 0), (0, 0), (0, 1), (2, 0), (2, 1)):
        conv.wait(dx, True, h)

    def mixed(buf, which, slot, rows):
        return jnp.dot(buf[slot, rows], obuf[which, slot], preferred_element_type=jnp.float32)

    oacc[...] = mixed(convg, 1, 0, slice(0, ROWS))

    @pl.loop(1, NTP)
    def _(slot):
        oacc[...] += mixed(convg, 1, slot, slice(0, ROWS))

    to = (at_y(1), at_y(3))
    near = (lax.rem(y + 1, NY), lax.rem(y + 3, NY))
    opposite = lax.rem(y + 2, NY)
    second = lax.broadcasted_iota(jnp.int32, (NY, LANES), 1) >= TILE

    def combined(h, block):
        part = a_ref[h * NY + block, :VDIM] * coef[h, pl.ds(block, 1)]
        return part[:, :TILE] + part[:, TILE:]

    def part_copy(h, k, target, device):
        n = 3 * h + k
        return remote(csend.at[n], target, c_send.at[n], c_recv.at[n], device)

    c_copies = [
        [
            part_copy(h, 0, crelay.at[h], to[h]),
            part_copy(h, 1, crecv.at[h, 0], to[1 - h]),
            part_copy(h, 2, crecv.at[h, 1], to[h]),
        ]
        for h in (0, 1)
    ]

    def weigh(h):
        for i in (1, 3, 2):
            peer = lax.rem(y + i, NY)
            remote(
                stg.at[peer, h], stg.at[peer, h], st_send.at[h, 0], st_recv.at[peer, h], at_y(1)
            ).wait_recv()
        m_all = stg[0, h, :NY]
        for i in range(1, NY):
            m_all = jnp.maximum(m_all, stg[i, h, :NY])
        l_all = stg[0, h, NY:] * jnp.exp2(stg[0, h, :NY] - m_all)
        for i in range(1, NY):
            l_all = l_all + stg[i, h, NY:] * jnp.exp2(stg[i, h, :NY] - m_all)
        share = jnp.exp2(stg[y, h, :NY] - m_all) / l_all
        coef[h, :NY] = jnp.where(second, -lam[0] * share, share)
        coef[h, NY:] = m_all * LN2 + jnp.log(l_all)
        csend[3 * h] = bf16(combined(h, opposite))
        c_copies[h][0].start()
        csend[3 * h + 1] = bf16(combined(h, near[1 - h]))
        c_copies[h][1].start()
        cown[:, h * TILE : (h + 1) * TILE] = combined(h, near[h])

    def pass_on(h):
        lanes = slice(h * TILE, (h + 1) * TILE)
        c_copies[h][0].wait_recv()
        csend[3 * h + 2] = bf16(cown[:, lanes] + f32(crelay[h]))
        c_copies[h][2].start()
        cown[:, lanes] = combined(h, y)
        row = coef[h, pl.ds(NY + y, 1)]
        logs[0, 0:1, lanes] = row[:, :TILE]
        logs[0, 1:2, lanes] = row[:, TILE:]

    def settle(h):
        c_copies[h][1].wait_recv()
        c_copies[h][2].wait_recv()
        head_mix = cown[:, h * TILE : (h + 1) * TILE] + f32(crecv[h, 0]) + f32(crecv[h, 1])
        mean = jnp.sum(head_mix * head_mix, axis=0, keepdims=True) / VDIM
        normed = jnp.transpose(head_mix * lax.rsqrt(mean + HEAD_EPS))
        attng[tp, h * HALF : (h + 1) * HALF] = bf16(normed * head_gain[...] * HEAD_SCALE)
        attn.start(2 * h)

    for stage in (weigh, pass_on, settle):
        for h in (0, 1):
            stage(h)

    def add(slot, h):
        rows = slice(h * HALF, (h + 1) * HALF)
        oacc[rows] += mixed(attng, 0, slot, rows)

    add(tp, 0)
    add(tp, 1)
    gathered(attn, add)
    out[...] = bf16(oacc[...])

    tokens.finish()
    for d in range(NZ // 2):
        k_copy(z, ku_send.at[d], at_z(1)).wait_send()
        v_copy(z, vd_send.at[d], at_z(-1)).wait_send()
        if d < NZ // 2 - 1:
            k_copy(z, kd_send.at[d], at_z(-1)).wait_send()
            v_copy(z, vu_send.at[d], at_z(1)).wait_send()
    for copy in q_copies + c_copies[0] + c_copies[1] + [tail]:
        copy.wait_send()
    for h in (0, 1):
        for i in (1, 2, 3):
            st_copy(h, i).wait_send()
    conv.finish()
    attn.finish()


def per_device(
    tokens,
    norm_gain,
    query_weight,
    key_weight,
    value_weight,
    outer_gate_weight,
    inner_gate_weight,
    conv_input_weight,
    conv_taps,
    lambdas,
    head_gain,
    attn_out_weight,
    conv_out_weight,
):
    half = DIM // 2
    frequency = np.float32(ROPE_BASE) ** (-np.arange(half, dtype=np.float32) * 2.0 / DIM)
    frequency = np.tile(frequency.astype(np.float64), 4)
    sign = np.tile(np.repeat([-1.0, 1.0], half), 2)
    start = np.arange(NY * NZ)[:, None] * ROWS * frequency
    cosine, sine = np.cos(start), np.sin(start)
    base = np.stack([cosine, sine, sign * cosine, sign * sine], axis=1).astype(np.float32)
    row = np.arange(ROWS)[:, None] * frequency
    rows = np.stack([np.cos(row), np.sin(row)]).astype(np.float32)

    def in_pieces(weight):
        return weight.reshape(NTP, PIECE, VDIM)

    vmem = pl.BlockSpec(memory_space=pltpu.VMEM)
    anywhere = pl.BlockSpec(memory_space=pltpu.HBM)
    dma = pltpu.SemaphoreType.DMA
    bf, fl = jnp.bfloat16, jnp.float32
    mixed_out, logs = pl.pallas_call(
        kernel,
        out_shape=(
            jax.ShapeDtypeStruct((ROWS, PIECE), bf),
            jax.ShapeDtypeStruct((1, 2, ROWS), fl),
        ),
        in_specs=[anywhere] * 15,
        out_specs=(vmem, vmem),
        scratch_shapes=[
            pltpu.VMEM((ROWS, PIECE), bf),
            pltpu.VMEM((NTP, 1, PIECE), fl),
            pltpu.VMEM((4, 128), fl),
            pltpu.VMEM((2, ROWS, 128), fl),
            pltpu.VMEM((3, VDIM), fl),
            pltpu.SMEM((1,), fl),
            pltpu.VMEM((1, VDIM), fl),
            pltpu.VMEM((NTP, ROWS, PIECE), bf),
            pltpu.VMEM((NTP, PIECE, 6 * VDIM), bf),
            pltpu.VMEM((2, NTP, VDIM, PIECE), bf),
            pltpu.VMEM((ROWS, 6 * VDIM), fl),
            pltpu.VMEM((ROWS, 128), fl),
            pltpu.VMEM((NZ, ROWS, VDIM), bf),
            pltpu.VMEM((NZ, VDIM, ROWS), bf),
            pltpu.VMEM((NY, VDIM, ROWS), bf),
            pltpu.VMEM((TILES, 2 * VDIM, LANES), bf),
            pltpu.VMEM((TILES, 1, LANES), fl),
            pltpu.VMEM((TILES, VDIM + ONES_ROWS, LANES), fl),
            pltpu.VMEM((2, ROWS, LANES), fl),
            pltpu.VMEM((NY, 2, TILES, LANES), fl),
            pltpu.VMEM((2, TILES, LANES), fl),
            pltpu.VMEM((6, VDIM, TILE), bf),
            pltpu.VMEM((2, VDIM, TILE), bf),
            pltpu.VMEM((2, 2, VDIM, TILE), bf),
            pltpu.VMEM((VDIM, ROWS), fl),
            pltpu.VMEM((ROWS, VDIM), fl),
            pltpu.VMEM((8 + ROWS, VDIM), fl),
            pltpu.VMEM((16, VDIM), bf),
            pltpu.VMEM((16, VDIM), bf),
            pltpu.VMEM((NTP, ROWS, VDIM), bf),
            pltpu.VMEM((NTP, ROWS, VDIM), bf),
            pltpu.VMEM((ROWS, PIECE), fl),
            dma((8,)),
            dma((7,)),
            dma((14,)),
            dma((NTP, 2)),
            dma((NZ // 2,)),
            dma((NZ // 2,)),
            dma((NZ // 2,)),
            dma((NZ // 2,)),
            dma((NZ,)),
            dma((NZ,)),
            dma((NY,)),
            dma((NY,)),
            dma((2, NY)),
            dma((NY, 2)),
            dma((6,)),
            dma((6,)),
            dma,
            dma,
            dma((14,)),
            dma((NTP, 2)),
            dma((28,)),
            dma((NTP, 4)),
        ],
        compiler_params=pltpu.CompilerParams(
            collective_id=0, has_side_effects=True, vmem_limit_bytes=60 * 2**20
        ),
    )(
        tokens,
        norm_gain.reshape(NTP, 1, PIECE),
        *(
            in_pieces(w)
            for w in (
                query_weight,
                key_weight,
                value_weight,
                outer_gate_weight,
                inner_gate_weight,
                conv_input_weight,
            )
        ),
        jnp.asarray(base),
        jnp.asarray(rows),
        conv_taps,
        lambdas,
        head_gain.reshape(1, VDIM),
        attn_out_weight.reshape(NTP, VDIM, PIECE),
        conv_out_weight.reshape(NTP, VDIM, PIECE),
    )
    return mixed_out, logs


def solution(mesh):
    in_specs = (
        P("sp", "tp"),
        P(),
        P(None, "tp"),
        P(None, "tp"),
        P(None, "tp"),
        P(None, "tp"),
        P(None, "tp"),
        P(None, "tp"),
        P(None, "tp"),
        P("tp"),
        P(),
        P(None, "tp"),
        P(None, "tp"),
    )
    out_specs = (P("sp", "tp"), P("tp", None, "sp"))
    return jax.shard_map(
        per_device, mesh=mesh, in_specs=in_specs, out_specs=out_specs, check_vma=False
    )
```

```python
import math

import jax
import jax.numpy as jnp
import numpy as np
from jax import lax
from jax.experimental import pallas as pl
from jax.experimental.pallas import tpu as pltpu
from jax.sharding import PartitionSpec as P

NORM_EPS = 1e-06
HEAD_EPS = 1e-05
ROPE_BASE = 500000.0
MASKED = -1e30
HEAD_SCALE = 0.8
MESH = pl.DeviceIdType.MESH

NY, NZ, NX, CORES = 4, 8, 4, 2
NTP = NX * CORES
ROWS = 512
HALF = ROWS // 2
PIECE = 256
DIM = 64
VDIM = 128
TILE = 256
LANES = 2 * TILE
TILES = NY * ROWS // TILE
ONES_ROWS = 16
LOG2E = math.log2(math.e)
LN2 = math.log(2.0)


def f32(x):
    return x.astype(jnp.float32)


def bf16(x):
    return x.astype(jnp.bfloat16)


def remote(src, dst, send_sem, recv_sem, device):
    return pltpu.make_async_remote_copy(
        src_ref=src,
        dst_ref=dst,
        send_sem=send_sem,
        recv_sem=recv_sem,
        device_id=device,
        device_id_type=MESH,
    )


class TpGather:
    def __init__(self, own, buf, send, recv, parts, sp, x, c):
        self.own, self.buf, self.send, self.recv, self.parts = own, buf, send, recv, parts
        self.slot = lambda dx, other: lax.rem(x + dx + NX, NX) * CORES + (1 - c if other else c)
        self.partner = (sp, x * CORES + 1 - c)
        self.right = (sp, self.slot(1, False))
        self.left = (sp, self.slot(-1, False))
        self.started = 0

    def rows(self, p):
        size = self.buf.shape[1] // self.parts
        return pl.ds(p * size, size)

    def push(self, dx, p, device, first=False):
        slot = self.slot(dx, False)
        block = self.buf.at[slot, self.rows(p)]
        source = self.own.at[self.rows(p)] if first else block
        remote(source, block, self.send.at[self.started], self.recv.at[slot, p], device).start()
        self.started += 1

    def wait(self, dx, other, *parts):
        slot = self.slot(dx, other)
        for p in parts:
            block = self.buf.at[slot, self.rows(p)]
            remote(block, block, self.send.at[0], self.recv.at[slot, p], self.partner).wait_recv()

    def start(self, *pairs):
        for p in pairs:
            self.push(0, p, self.right, True)
            self.push(0, p + 1, self.left, True)
        for p in pairs:
            self.push(0, p + 1, self.right, True)
            self.push(0, p, self.left, True)
        for p in pairs:
            self.push(0, p, self.partner, True)
            self.push(0, p + 1, self.partner, True)

    def neighbours_first(self, *pairs):
        for p in pairs:
            self.wait(-1, False, p)
            self.push(-1, p, self.right)
            self.wait(1, False, p + 1)
            self.push(1, p + 1, self.left)
        for p in pairs:
            self.push(-1, p, self.partner)
            self.push(1, p + 1, self.partner)

    def neighbours_second(self, *pairs):
        for p in pairs:
            self.wait(-1, False, p + 1)
            self.push(-1, p + 1, self.partner)
            self.wait(1, False, p)
            self.push(1, p, self.partner)

    def opposite(self, *parts):
        for p in parts:
            self.wait(2, False, p)
            self.push(2, p, self.partner)

    def finish(self):
        block = self.buf.at[0, self.rows(0)]
        for i in range(self.started):
            remote(block, block, self.send.at[i], self.recv.at[0, 0], self.partner).wait_send()


def kernel(
    tok_in, gain_in, wq, wk, wv, wo, wi, ws, base_in, rows_in, taps_in, lam_in, head_gain_in,
    wattn, wconv,
    out, logs,
    tok, gain, base, turn, taps, lam, head_gain, tbuf, wbuf, obuf, acc, ssq, kbuf, vbuf, qbuf, qbd, m_ref, a_ref, s_ref, stg, coef,
    csend, crelay, crecv, cown, ogate, cpad, tail_out, tail_in, convg, attng, oacc,
    w_sem, i_sem, t_send, t_recv, ku_send, kd_send, vu_send, vd_send, k_recv, v_recv,
    q_send, q_recv, st_send, st_recv, c_send, c_recv, h_send, h_recv,
    g_send, g_recv, a_send, a_recv,
):
    sp, tp = lax.axis_index("sp"), lax.axis_index("tp")
    z, y = sp // NY, lax.rem(sp, NY)
    x, c = tp // CORES, lax.rem(tp, CORES)

    def at_y(step):
        return (z * NY + lax.rem(y + step, NY), tp)

    def at_z(step):
        return (lax.rem(z + step + NZ, NZ) * NY + y, tp)

    after = (lax.rem(sp + 1, NY * NZ), tp)
    before = (lax.rem(sp + NY * NZ - 1, NY * NZ), tp)

    tokens = TpGather(tok, tbuf, t_send, t_recv, 2, sp, x, c)
    conv = TpGather(convg.at[tp], convg, g_send, g_recv, 2, sp, x, c)
    attn = TpGather(attng.at[tp], attng, a_send, a_recv, 4, sp, x, c)

    barrier = pltpu.get_barrier_semaphore()
    for device in (
        tokens.partner, tokens.left, tokens.right, at_y(1), at_y(2), at_y(3), at_z(1), at_z(-1), before,
    ):
        pl.semaphore_signal(barrier, inc=1, device_id=device, device_id_type=MESH)

    inputs = [
        pltpu.make_async_copy(source, target, i_sem.at[i])
        for i, (source, target) in enumerate(
            (
                (tok_in, tok),
                (gain_in, gain),
                (base_in.at[sp], base),
                (rows_in, turn),
                (taps_in, taps),
                (lam_in, lam),
                (head_gain_in, head_gain),
            )
        )
    ]
    loads = [
        pltpu.make_async_copy(w, wbuf.at[:, :, i * VDIM : (i + 1) * VDIM], w_sem.at[i])
        for i, w in enumerate((wq, wk, wv, wo, wi, ws))
    ]
    loads += [
        pltpu.make_async_copy(w, obuf.at[i], w_sem.at[6 + i]) for i, w in enumerate((wattn, wconv))
    ]
    for load in inputs + loads:
        load.start()
    inputs[0].wait()
    pl.semaphore_wait(barrier, 9)

    tokens.start(0)

    m_ref[...] = jnp.full_like(m_ref, MASKED)
    a_ref[...] = jnp.zeros_like(a_ref)
    qbd[...] = jnp.zeros_like(qbd)
    acc[...] = jnp.zeros_like(acc)
    ssq[...] = jnp.zeros_like(ssq)
    for load in inputs[1:] + loads[:6]:
        load.wait()

    block_cos, block_sin, signed_cos, signed_sin = (base[i : i + 1] for i in range(4))
    row_cos, row_sin = turn[0], turn[1]
    turn[0] = block_cos * row_cos - block_sin * row_sin
    turn[1] = signed_sin * row_cos + signed_cos * row_sin

    def project(slot, h, src=None):
        rows = slice(h * HALF, (h + 1) * HALF)
        block = f32(tbuf[slot, rows] if src is None else src[rows])
        square = block * block
        ssq[rows] += square[:, :128] + square[:, 128:]
        scaled = bf16(block * gain[slot])
        acc[rows] += jnp.dot(scaled, wbuf[slot], preferred_element_type=jnp.float32)

    def gathered(gather, use):
        each = gather.parts // 2
        halves = (range(each), range(each, 2 * each))
        pairs = range(0, gather.parts, 2)
        for h in (0, 1):
            gather.wait(0, True, *halves[h])
            use(gather.slot(0, True), h)
        gather.neighbours_first(*pairs)
        gather.neighbours_second(*pairs)
        for dx in (-1, 1):
            for h in (0, 1):
                use(gather.slot(dx, False), h)
        for dx in (-1, 1):
            for h in (0, 1):
                gather.wait(dx, True, *halves[h])
                use(gather.slot(dx, True), h)
        gather.opposite(*halves[0], *halves[1])
        for other in (False, True):
            for h in (0, 1):
                if other:
                    gather.wait(2, True, *halves[h])
                use(gather.slot(2, other), h)

    project(tp, 0, tok)
    project(tp, 1, tok)
    gathered(tokens, project)

    total = jnp.sum(ssq[...], axis=1, keepdims=True)
    inverse_rms = lax.rsqrt(total / (NTP * PIECE) + NORM_EPS)

    def projected(i):
        return inverse_rms * acc[:, i * VDIM : (i + 1) * VDIM]

    first_half = lax.rem(lax.broadcasted_iota(jnp.int32, (ROWS, VDIM), 1), DIM) < DIM // 2

    def turned(field):
        other = jnp.where(
            first_half, pltpu.roll(field, VDIM - DIM // 2, 1), pltpu.roll(field, DIM // 2, 1)
        )
        return field * turn[0] + other * turn[1]

    kbuf[z] = bf16(turned(projected(1)))
    vbuf[z] = bf16(jnp.transpose(projected(2)))

    def k_copy(slot, send_sem, device):
        return remote(kbuf.at[slot], kbuf.at[slot], send_sem, k_recv.at[slot], device)

    def v_copy(slot, send_sem, device):
        return remote(vbuf.at[slot], vbuf.at[slot], send_sem, v_recv.at[slot], device)

    k_copy(z, ku_send.at[0], at_z(1)).start()
    k_copy(z, kd_send.at[0], at_z(-1)).start()
    v_copy(z, vu_send.at[0], at_z(1)).start()
    v_copy(z, vd_send.at[0], at_z(-1)).start()

    qbuf[y] = bf16(jnp.transpose(turned(projected(0))))
    q_copies = [
        remote(qbuf.at[y], qbuf.at[y], q_send.at[i - 1], q_recv.at[y], at_y(i)) for i in (1, 3, 2)
    ]
    for copy in q_copies:
        copy.start()

    ogate[...] = f32(bf16(projected(3)))
    conv_in = bf16(f32(bf16(projected(4))) * f32(bf16(projected(5))))
    cpad[8:] = f32(conv_in)
    tail_out[...] = conv_in[ROWS - 16 :]
    tail = remote(tail_out, tail_in, h_send, h_recv, after)
    tail.start()

    def blocked(block):
        scaled = f32(qbuf[block]) * (LOG2E * DIM**-0.5)
        high = bf16(scaled)
        low = bf16(scaled - f32(high))
        for h in (0, 1):
            lanes = slice(h * TILE, (h + 1) * TILE)
            for t, term in enumerate((high, low)):
                qbd[h * NY + block, t * VDIM : t * VDIM + DIM, :TILE] = term[:DIM, lanes]
                qbd[h * NY + block, t * VDIM + DIM : (t + 1) * VDIM, TILE:] = term[DIM:, lanes]

    ones = jnp.ones((ONES_ROWS, ROWS), jnp.bfloat16)

    def scores(slot, tile, count=ROWS):
        keys = kbuf[slot, :count]
        return jnp.dot(
            jnp.concatenate([keys, keys], axis=1), qbd[tile], preferred_element_type=jnp.float32
        )

    def absorb(slot, tile, s, count=ROWS):
        m_old = m_ref[tile]
        m_new = jnp.maximum(m_old, jnp.max(s, axis=0, keepdims=True))
        keep = jnp.exp2(m_old - m_new)
        m_ref[tile] = m_new
        weights = bf16(jnp.exp2(s - m_new))
        a_ref[tile] = a_ref[tile] * keep + jnp.dot(
            jnp.concatenate([vbuf[slot, :, :count], ones[:, :count]], axis=0),
            weights,
            preferred_element_type=jnp.float32,
        )

    def four_tiles(slot, g):
        for i in range(4):
            tile = g * 4 + i
            s_ref[(i + 1) % 2] = scores(slot, lax.rem(tile + 1, TILES))
            absorb(slot, tile, s_ref[i % 2])

    blocked(y)
    for h in (0, 1):
        count = (h + 1) * TILE
        key_pos = lax.broadcasted_iota(jnp.int32, (count, LANES), 0)
        query_pos = lax.rem(lax.broadcasted_iota(jnp.int32, (count, LANES), 1), TILE) + h * TILE
        s = jnp.where(key_pos <= query_pos, scores(z, h * NY + y, count), MASKED)
        absorb(z, h * NY + y, s, count)

    last = NZ // 2

    def pass_keys(d):
        below, above = lax.rem(z - d + NZ, NZ), lax.rem(z + d, NZ)
        k_copy(below, ku_send.at[0], at_z(1)).wait_recv()

        @pl.when(d < last)
        def _():
            k_copy(below, ku_send.at[d], at_z(1)).start()
            k_copy(above, ku_send.at[0], at_z(1)).wait_recv()

        @pl.when(d < last - 1)
        def _():
            k_copy(above, kd_send.at[d], at_z(-1)).start()

    def pass_values(d):
        below, above = lax.rem(z - d + NZ, NZ), lax.rem(z + d, NZ)
        v_copy(above, vu_send.at[0], at_z(1)).wait_recv()

        @pl.when(d < last)
        def _():
            v_copy(above, vd_send.at[d], at_z(-1)).start()
            v_copy(below, vu_send.at[0], at_z(1)).wait_recv()

        @pl.when(d < last - 1)
        def _():
            v_copy(below, vu_send.at[d], at_z(1)).start()

    pass_keys(1)

    for i in (1, 3, 2):
        block = lax.rem(y + i, NY)
        remote(qbuf.at[block], qbuf.at[block], q_send.at[0], q_recv.at[block], at_y(1)).wait_recv()
        blocked(block)

    pass_values(1)

    @pl.when(y < NY - 1)
    def _():
        s_ref[0] = scores(z, y + 1)

        @pl.loop(y + 1, NY)
        def _(block):
            s_ref[1] = scores(z, NY + block)
            absorb(z, block, s_ref[0])
            s_ref[0] = scores(z, lax.rem(block + 1, NY))
            absorb(z, NY + block, s_ref[1])

    tail.wait_recv()
    rim = f32(tail_in[8:])
    cpad[:8] = jnp.where(sp > 0, rim, jnp.zeros_like(rim))
    summed = taps[0:1] * cpad[6 : 6 + ROWS]
    summed += taps[1:2] * cpad[7 : 7 + ROWS]
    summed += taps[2:3] * cpad[8 : 8 + ROWS]
    convg[tp] = bf16(ogate[...] * summed)
    conv.start(0)

    def half_block(source, g):
        @pl.when((source < z) & (g == 0))
        def _():
            s_ref[0] = scores(source, 0)

        @pl.when(source < z)
        def _():
            four_tiles(source, g)

    @pl.loop(0, NZ - 2)
    def _(i):
        d, r = i // 2 + 1, lax.rem(i, 2)
        source = lax.rem(z + jnp.where(r == 0, NZ - d, d), NZ)

        @pl.loop(0, 2)
        def _(g):
            @pl.when((g == 1) & (r == 0))
            def _():
                pass_keys(d + 1)

            @pl.when((g == 1) & (r == 1))
            def _():
                pass_values(d + 1)

            half_block(source, g)

        @pl.when(i == 1)
        def _():
            conv.neighbours_first(0)
            conv.neighbours_second(0)

        @pl.when(i == 3)
        def _():
            conv.opposite(0, 1)

    def st_copy(h, i):
        return remote(stg.at[y, h], stg.at[y, h], st_send.at[h, i - 1], st_recv.at[y, h], at_y(i))

    @pl.loop(0, 2)
    def _(h):
        half_block(lax.rem(z + last, NZ), h)
        for t in range(NY):
            stg[y, h, t : t + 1] = m_ref[h * NY + t]
            stg[y, h, NY + t : NY + t + 1] = a_ref[h * NY + t, VDIM : VDIM + 1]
        for i in (2, 1, 3):
            st_copy(h, i).start()

    for load in loads[6:]:
        load.wait()
    for dx, h in ((-1, 0), (1, 1), (-1, 1), (1, 0), (0, 0), (0, 1), (2, 0), (2, 1)):
        conv.wait(dx, True, h)

    def mixed(buf, which, slot, rows):
        return jnp.dot(buf[slot, rows], obuf[which, slot], preferred_element_type=jnp.float32)

    oacc[...] = mixed(convg, 1, 0, slice(0, ROWS))

    @pl.loop(1, NTP)
    def _(slot):
        oacc[...] += mixed(convg, 1, slot, slice(0, ROWS))

    to = (at_y(1), at_y(3))
    near = (lax.rem(y + 1, NY), lax.rem(y + 3, NY))
    opposite = lax.rem(y + 2, NY)
    second = lax.broadcasted_iota(jnp.int32, (NY, LANES), 1) >= TILE

    def combined(h, block):
        part = a_ref[h * NY + block, :VDIM] * coef[h, pl.ds(block, 1)]
        return part[:, :TILE] + part[:, TILE:]

    def part_copy(h, k, target, device):
        n = 3 * h + k
        return remote(csend.at[n], target, c_send.at[n], c_recv.at[n], device)

    c_copies = [
        [
            part_copy(h, 0, crelay.at[h], to[h]),
            part_copy(h, 1, crecv.at[h, 0], to[1 - h]),
            part_copy(h, 2, crecv.at[h, 1], to[h]),
        ]
        for h in (0, 1)
    ]

    def weigh(h):
        for i in (1, 3, 2):
            peer = lax.rem(y + i, NY)
            remote(
                stg.at[peer, h], stg.at[peer, h], st_send.at[h, 0], st_recv.at[peer, h], at_y(1)
            ).wait_recv()
        m_all = stg[0, h, :NY]
        for i in range(1, NY):
            m_all = jnp.maximum(m_all, stg[i, h, :NY])
        l_all = stg[0, h, NY:] * jnp.exp2(stg[0, h, :NY] - m_all)
        for i in range(1, NY):
            l_all = l_all + stg[i, h, NY:] * jnp.exp2(stg[i, h, :NY] - m_all)
        share = jnp.exp2(stg[y, h, :NY] - m_all) / l_all
        coef[h, :NY] = jnp.where(second, -lam[0] * share, share)
        coef[h, NY:] = m_all * LN2 + jnp.log(l_all)
        csend[3 * h] = bf16(combined(h, opposite))
        c_copies[h][0].start()
        csend[3 * h + 1] = bf16(combined(h, near[1 - h]))
        c_copies[h][1].start()
        cown[:, h * TILE : (h + 1) * TILE] = combined(h, near[h])

    def pass_on(h):
        lanes = slice(h * TILE, (h + 1) * TILE)
        c_copies[h][0].wait_recv()
        csend[3 * h + 2] = bf16(cown[:, lanes] + f32(crelay[h]))
        c_copies[h][2].start()
        cown[:, lanes] = combined(h, y)
        row = coef[h, pl.ds(NY + y, 1)]
        logs[0, 0:1, lanes] = row[:, :TILE]
        logs[0, 1:2, lanes] = row[:, TILE:]

    def settle(h):
        c_copies[h][1].wait_recv()
        c_copies[h][2].wait_recv()
        head_mix = cown[:, h * TILE : (h + 1) * TILE] + f32(crecv[h, 0]) + f32(crecv[h, 1])
        mean = jnp.sum(head_mix * head_mix, axis=0, keepdims=True) / VDIM
        normed = jnp.transpose(head_mix * lax.rsqrt(mean + HEAD_EPS))
        attng[tp, h * HALF : (h + 1) * HALF] = bf16(normed * head_gain[...] * HEAD_SCALE)
        attn.start(2 * h)

    for stage in (weigh, pass_on, settle):
        for h in (0, 1):
            stage(h)

    def add(slot, h):
        rows = slice(h * HALF, (h + 1) * HALF)
        oacc[rows] += mixed(attng, 0, slot, rows)

    add(tp, 0)
    add(tp, 1)
    gathered(attn, add)
    out[...] = bf16(oacc[...])

    tokens.finish()
    for d in range(NZ // 2):
        k_copy(z, ku_send.at[d], at_z(1)).wait_send()
        v_copy(z, vd_send.at[d], at_z(-1)).wait_send()
        if d < NZ // 2 - 1:
            k_copy(z, kd_send.at[d], at_z(-1)).wait_send()
            v_copy(z, vu_send.at[d], at_z(1)).wait_send()
    for copy in q_copies + c_copies[0] + c_copies[1] + [tail]:
        copy.wait_send()
    for h in (0, 1):
        for i in (1, 2, 3):
            st_copy(h, i).wait_send()
    conv.finish()
    attn.finish()


def per_device(
    tokens,
    norm_gain,
    query_weight,
    key_weight,
    value_weight,
    outer_gate_weight,
    inner_gate_weight,
    conv_input_weight,
    conv_taps,
    lambdas,
    head_gain,
    attn_out_weight,
    conv_out_weight,
):
    half = DIM // 2
    frequency = np.float32(ROPE_BASE) ** (-np.arange(half, dtype=np.float32) * 2.0 / DIM)
    frequency = np.tile(frequency.astype(np.float64), 4)
    sign = np.tile(np.repeat([-1.0, 1.0], half), 2)
    start = np.arange(NY * NZ)[:, None] * ROWS * frequency
    cosine, sine = np.cos(start), np.sin(start)
    base = np.stack([cosine, sine, sign * cosine, sign * sine], axis=1).astype(np.float32)
    row = np.arange(ROWS)[:, None] * frequency
    rows = np.stack([np.cos(row), np.sin(row)]).astype(np.float32)

    def in_pieces(weight):
        return weight.reshape(NTP, PIECE, VDIM)

    vmem = pl.BlockSpec(memory_space=pltpu.VMEM)
    anywhere = pl.BlockSpec(memory_space=pltpu.HBM)
    dma = pltpu.SemaphoreType.DMA
    bf, fl = jnp.bfloat16, jnp.float32
    mixed_out, logs = pl.pallas_call(
        kernel,
        out_shape=(
            jax.ShapeDtypeStruct((ROWS, PIECE), bf),
            jax.ShapeDtypeStruct((1, 2, ROWS), fl),
        ),
        in_specs=[anywhere] * 15,
        out_specs=(vmem, vmem),
        scratch_shapes=[
            pltpu.VMEM((ROWS, PIECE), bf),
            pltpu.VMEM((NTP, 1, PIECE), fl),
            pltpu.VMEM((4, 128), fl),
            pltpu.VMEM((2, ROWS, 128), fl),
            pltpu.VMEM((3, VDIM), fl),
            pltpu.SMEM((1,), fl),
            pltpu.VMEM((1, VDIM), fl),
            pltpu.VMEM((NTP, ROWS, PIECE), bf),
            pltpu.VMEM((NTP, PIECE, 6 * VDIM), bf),
            pltpu.VMEM((2, NTP, VDIM, PIECE), bf),
            pltpu.VMEM((ROWS, 6 * VDIM), fl),
            pltpu.VMEM((ROWS, 128), fl),
            pltpu.VMEM((NZ, ROWS, VDIM), bf),
            pltpu.VMEM((NZ, VDIM, ROWS), bf),
            pltpu.VMEM((NY, VDIM, ROWS), bf),
            pltpu.VMEM((TILES, 2 * VDIM, LANES), bf),
            pltpu.VMEM((TILES, 1, LANES), fl),
            pltpu.VMEM((TILES, VDIM + ONES_ROWS, LANES), fl),
            pltpu.VMEM((2, ROWS, LANES), fl),
            pltpu.VMEM((NY, 2, TILES, LANES), fl),
            pltpu.VMEM((2, TILES, LANES), fl),
            pltpu.VMEM((6, VDIM, TILE), bf),
            pltpu.VMEM((2, VDIM, TILE), bf),
            pltpu.VMEM((2, 2, VDIM, TILE), bf),
            pltpu.VMEM((VDIM, ROWS), fl),
            pltpu.VMEM((ROWS, VDIM), fl),
            pltpu.VMEM((8 + ROWS, VDIM), fl),
            pltpu.VMEM((16, VDIM), bf),
            pltpu.VMEM((16, VDIM), bf),
            pltpu.VMEM((NTP, ROWS, VDIM), bf),
            pltpu.VMEM((NTP, ROWS, VDIM), bf),
            pltpu.VMEM((ROWS, PIECE), fl),
            dma((8,)),
            dma((7,)),
            dma((14,)),
            dma((NTP, 2)),
            dma((NZ // 2,)),
            dma((NZ // 2,)),
            dma((NZ // 2,)),
            dma((NZ // 2,)),
            dma((NZ,)),
            dma((NZ,)),
            dma((NY,)),
            dma((NY,)),
            dma((2, NY)),
            dma((NY, 2)),
            dma((6,)),
            dma((6,)),
            dma,
            dma,
            dma((14,)),
            dma((NTP, 2)),
            dma((28,)),
            dma((NTP, 4)),
        ],
        compiler_params=pltpu.CompilerParams(
            collective_id=0, has_side_effects=True, vmem_limit_bytes=40 * 2**20
        ),
    )(*(v if v is lambdas else pltpu.with_memory_space_constraint(v, pltpu.HBM) for v in (
        tokens,
        norm_gain.reshape(NTP, 1, PIECE),
        *(
            in_pieces(w)
            for w in (
                query_weight,
                key_weight,
                value_weight,
                outer_gate_weight,
                inner_gate_weight,
                conv_input_weight,
            )
        ),
        jnp.asarray(base),
        jnp.asarray(rows),
        conv_taps,
        lambdas,
        head_gain.reshape(1, VDIM),
        attn_out_weight.reshape(NTP, VDIM, PIECE),
        conv_out_weight.reshape(NTP, VDIM, PIECE),
    )))
    return mixed_out, logs


def solution(mesh):
    in_specs = (
        P("sp", "tp"),
        P(),
        P(None, "tp"),
        P(None, "tp"),
        P(None, "tp"),
        P(None, "tp"),
        P(None, "tp"),
        P(None, "tp"),
        P(None, "tp"),
        P("tp"),
        P(),
        P(None, "tp"),
        P(None, "tp"),
    )
    out_specs = (P("sp", "tp"), P("tp", None, "sp"))
    return jax.shard_map(
        per_device, mesh=mesh, in_specs=in_specs, out_specs=out_specs, check_vma=False
    )
```

```python
import math

import jax
import jax.numpy as jnp
import numpy as np
from jax import lax
from jax.experimental import pallas as pl
from jax.experimental.pallas import tpu as pltpu
from jax.sharding import PartitionSpec as P

NORM_EPS = 1e-06
HEAD_EPS = 1e-05
ROPE_BASE = 500000.0
MASKED = -1e30
HEAD_SCALE = 0.8
MESH = pl.DeviceIdType.MESH

NY, NZ, NX, CORES = 4, 8, 4, 2
NTP = NX * CORES
ROWS = 512
HALF = ROWS // 2
PIECE = 256
DIM = 64
VDIM = 128
TILE = 256
LANES = 2 * TILE
TILES = NY * ROWS // TILE
ONES_ROWS = 16
LOG2E = math.log2(math.e)
LN2 = math.log(2.0)


def f32(x):
    return x.astype(jnp.float32)


def bf16(x):
    return x.astype(jnp.bfloat16)


def remote(src, dst, send_sem, recv_sem, device):
    return pltpu.make_async_remote_copy(
        src_ref=src,
        dst_ref=dst,
        send_sem=send_sem,
        recv_sem=recv_sem,
        device_id=device,
        device_id_type=MESH,
    )


class TpGather:
    def __init__(self, own, buf, send, recv, parts, sp, x, c):
        self.own, self.buf, self.send, self.recv, self.parts = own, buf, send, recv, parts
        self.slot = lambda dx, other: lax.rem(x + dx + NX, NX) * CORES + (1 - c if other else c)
        self.partner = (sp, x * CORES + 1 - c)
        self.right = (sp, self.slot(1, False))
        self.left = (sp, self.slot(-1, False))
        self.started = 0

    def rows(self, p):
        size = self.buf.shape[1] // self.parts
        return pl.ds(p * size, size)

    def push(self, dx, p, device, first=False):
        slot = self.slot(dx, False)
        block = self.buf.at[slot, self.rows(p)]
        source = self.own.at[self.rows(p)] if first else block
        remote(source, block, self.send.at[self.started], self.recv.at[slot, p], device).start()
        self.started += 1

    def wait(self, dx, other, *parts):
        slot = self.slot(dx, other)
        for p in parts:
            block = self.buf.at[slot, self.rows(p)]
            remote(block, block, self.send.at[0], self.recv.at[slot, p], self.partner).wait_recv()

    def start(self, *pairs):
        for p in pairs:
            self.push(0, p, self.right, True)
            self.push(0, p + 1, self.left, True)
        for p in pairs:
            self.push(0, p + 1, self.right, True)
            self.push(0, p, self.left, True)
        for p in pairs:
            self.push(0, p, self.partner, True)
            self.push(0, p + 1, self.partner, True)

    def neighbours_first(self, *pairs):
        for p in pairs:
            self.wait(-1, False, p)
            self.push(-1, p, self.right)
            self.wait(1, False, p + 1)
            self.push(1, p + 1, self.left)
        for p in pairs:
            self.push(-1, p, self.partner)
            self.push(1, p + 1, self.partner)

    def neighbours_second(self, *pairs):
        for p in pairs:
            self.wait(-1, False, p + 1)
            self.push(-1, p + 1, self.partner)
            self.wait(1, False, p)
            self.push(1, p, self.partner)

    def opposite(self, *parts):
        for p in parts:
            self.wait(2, False, p)
            self.push(2, p, self.partner)

    def finish(self):
        block = self.buf.at[0, self.rows(0)]
        for i in range(self.started):
            remote(block, block, self.send.at[i], self.recv.at[0, 0], self.partner).wait_send()


def kernel(
    tok_in, gain_in, wq, wk, wv, wo, wi, ws, base_in, rows_in, taps_in, lam_in, head_gain_in,
    wattn, wconv,
    out, logs,
    tok, gain, base, turn, taps, lam, head_gain, tbuf, wbuf, obuf, acc, ssq, kbuf, vbuf, qbuf, qbd, m_ref, a_ref, s_ref, stg, coef,
    csend, crelay, crecv, cown, ogate, cpad, tail_out, tail_in, convg, attng, oacc,
    w_sem, i_sem, t_send, t_recv, ku_send, kd_send, vu_send, vd_send, k_recv, v_recv,
    q_send, q_recv, st_send, st_recv, c_send, c_recv, h_send, h_recv,
    g_send, g_recv, a_send, a_recv,
):
    sp, tp = lax.axis_index("sp"), lax.axis_index("tp")
    z, y = sp // NY, lax.rem(sp, NY)
    x, c = tp // CORES, lax.rem(tp, CORES)

    def at_y(step):
        return (z * NY + lax.rem(y + step, NY), tp)

    def at_z(step):
        return (lax.rem(z + step + NZ, NZ) * NY + y, tp)

    after = (lax.rem(sp + 1, NY * NZ), tp)
    before = (lax.rem(sp + NY * NZ - 1, NY * NZ), tp)

    tokens = TpGather(tok, tbuf, t_send, t_recv, 2, sp, x, c)
    conv = TpGather(convg.at[tp], convg, g_send, g_recv, 2, sp, x, c)
    attn = TpGather(attng.at[tp], attng, a_send, a_recv, 4, sp, x, c)

    barrier = pltpu.get_barrier_semaphore()
    for device in (
        tokens.partner, tokens.left, tokens.right, at_y(1), at_y(2), at_y(3), at_z(1), at_z(-1), before,
    ):
        pl.semaphore_signal(barrier, inc=1, device_id=device, device_id_type=MESH)

    inputs = [
        pltpu.make_async_copy(source, target, i_sem.at[i])
        for i, (source, target) in enumerate(
            (
                (tok_in, tok),
                (gain_in, gain),
                (base_in.at[sp], base),
                (rows_in, turn),
                (taps_in, taps),
                (lam_in, lam),
                (head_gain_in, head_gain),
            )
        )
    ]
    loads = [
        pltpu.make_async_copy(w, wbuf.at[:, :, i * VDIM : (i + 1) * VDIM], w_sem.at[i])
        for i, w in enumerate((wq, wk, wv, wo, wi, ws))
    ]
    loads += [
        pltpu.make_async_copy(w, obuf.at[i], w_sem.at[6 + i]) for i, w in enumerate((wattn, wconv))
    ]
    for load in inputs + loads:
        load.start()
    inputs[0].wait()
    pl.semaphore_wait(barrier, 9)

    tokens.start(0)

    m_ref[...] = jnp.full_like(m_ref, MASKED)
    a_ref[...] = jnp.zeros_like(a_ref)
    qbd[...] = jnp.zeros_like(qbd)
    acc[...] = jnp.zeros_like(acc)
    ssq[...] = jnp.zeros_like(ssq)
    for load in inputs[1:] + loads[:6]:
        load.wait()

    block_cos, block_sin, signed_cos, signed_sin = (base[i : i + 1] for i in range(4))
    row_cos, row_sin = turn[0], turn[1]
    turn[0] = block_cos * row_cos - block_sin * row_sin
    turn[1] = signed_sin * row_cos + signed_cos * row_sin

    def project(slot, h, src=None):
        rows = slice(h * HALF, (h + 1) * HALF)
        block = f32(tbuf[slot, rows] if src is None else src[rows])
        square = block * block
        ssq[rows] += square[:, :128] + square[:, 128:]
        scaled = bf16(block * gain[slot])
        acc[rows] += jnp.dot(scaled, wbuf[slot], preferred_element_type=jnp.float32)

    def gathered(gather, use):
        each = gather.parts // 2
        halves = (range(each), range(each, 2 * each))
        pairs = range(0, gather.parts, 2)
        for h in (0, 1):
            gather.wait(0, True, *halves[h])
            use(gather.slot(0, True), h)
        gather.neighbours_first(*pairs)
        gather.neighbours_second(*pairs)
        for dx in (-1, 1):
            for h in (0, 1):
                use(gather.slot(dx, False), h)
        for dx in (-1, 1):
            for h in (0, 1):
                gather.wait(dx, True, *halves[h])
                use(gather.slot(dx, True), h)
        gather.opposite(*halves[0], *halves[1])
        for other in (False, True):
            for h in (0, 1):
                if other:
                    gather.wait(2, True, *halves[h])
                use(gather.slot(2, other), h)

    project(tp, 0, tok)
    project(tp, 1, tok)
    gathered(tokens, project)

    total = jnp.sum(ssq[...], axis=1, keepdims=True)
    inverse_rms = lax.rsqrt(total / (NTP * PIECE) + NORM_EPS)

    def projected(i):
        return inverse_rms * acc[:, i * VDIM : (i + 1) * VDIM]

    first_half = lax.rem(lax.broadcasted_iota(jnp.int32, (ROWS, VDIM), 1), DIM) < DIM // 2

    def turned(field):
        other = jnp.where(
            first_half, pltpu.roll(field, VDIM - DIM // 2, 1), pltpu.roll(field, DIM // 2, 1)
        )
        return field * turn[0] + other * turn[1]

    kbuf[z] = bf16(turned(projected(1)))
    vbuf[z] = bf16(jnp.transpose(projected(2)))

    def k_copy(slot, send_sem, device):
        return remote(kbuf.at[slot], kbuf.at[slot], send_sem, k_recv.at[slot], device)

    def v_copy(slot, send_sem, device):
        return remote(vbuf.at[slot], vbuf.at[slot], send_sem, v_recv.at[slot], device)

    k_copy(z, ku_send.at[0], at_z(1)).start()
    k_copy(z, kd_send.at[0], at_z(-1)).start()
    v_copy(z, vu_send.at[0], at_z(1)).start()
    v_copy(z, vd_send.at[0], at_z(-1)).start()

    qbuf[y] = bf16(jnp.transpose(turned(projected(0))))
    q_copies = [
        remote(qbuf.at[y], qbuf.at[y], q_send.at[i - 1], q_recv.at[y], at_y(i)) for i in (1, 3, 2)
    ]
    for copy in q_copies:
        copy.start()

    ogate[...] = f32(bf16(projected(3)))
    conv_in = bf16(f32(bf16(projected(4))) * f32(bf16(projected(5))))
    cpad[8:] = f32(conv_in)
    tail_out[...] = conv_in[ROWS - 16 :]
    tail = remote(tail_out, tail_in, h_send, h_recv, after)
    tail.start()

    def blocked(block):
        scaled = f32(qbuf[block]) * (LOG2E * DIM**-0.5)
        high = bf16(scaled)
        low = bf16(scaled - f32(high))
        for h in (0, 1):
            lanes = slice(h * TILE, (h + 1) * TILE)
            for t, term in enumerate((high, low)):
                qbd[h * NY + block, t * VDIM : t * VDIM + DIM, :TILE] = term[:DIM, lanes]
                qbd[h * NY + block, t * VDIM + DIM : (t + 1) * VDIM, TILE:] = term[DIM:, lanes]

    ones = jnp.ones((ONES_ROWS, ROWS), jnp.bfloat16)

    def scores(slot, tile, count=ROWS):
        keys = kbuf[slot, :count]
        return jnp.dot(
            jnp.concatenate([keys, keys], axis=1), qbd[tile], preferred_element_type=jnp.float32
        )

    def absorb(slot, tile, s, count=ROWS):
        m_old = m_ref[tile]
        m_new = jnp.maximum(m_old, jnp.max(s, axis=0, keepdims=True))
        keep = jnp.exp2(m_old - m_new)
        m_ref[tile] = m_new
        weights = bf16(jnp.exp2(s - m_new))
        a_ref[tile] = a_ref[tile] * keep + jnp.dot(
            jnp.concatenate([vbuf[slot, :, :count], ones[:, :count]], axis=0),
            weights,
            preferred_element_type=jnp.float32,
        )

    def four_tiles(slot, g):
        if g == 0:
            s_ref[0] = scores(slot, 0)
        for tile in range(4 * g, 4 * g + 4):
            if tile + 1 < TILES:
                s_ref[(tile + 1) % 2] = scores(slot, tile + 1)
            absorb(slot, tile, s_ref[tile % 2])

    blocked(y)
    for h in (0, 1):
        count = (h + 1) * TILE
        key_pos = lax.broadcasted_iota(jnp.int32, (count, LANES), 0)
        query_pos = lax.rem(lax.broadcasted_iota(jnp.int32, (count, LANES), 1), TILE) + h * TILE
        s = jnp.where(key_pos <= query_pos, scores(z, h * NY + y, count), MASKED)
        absorb(z, h * NY + y, s, count)

    last = NZ // 2

    def pass_keys(d):
        below, above = lax.rem(z - d + NZ, NZ), lax.rem(z + d, NZ)
        k_copy(below, ku_send.at[0], at_z(1)).wait_recv()

        @pl.when(d < last)
        def _():
            k_copy(below, ku_send.at[d], at_z(1)).start()
            k_copy(above, ku_send.at[0], at_z(1)).wait_recv()

        @pl.when(d < last - 1)
        def _():
            k_copy(above, kd_send.at[d], at_z(-1)).start()

    def pass_values(d):
        below, above = lax.rem(z - d + NZ, NZ), lax.rem(z + d, NZ)
        v_copy(above, vu_send.at[0], at_z(1)).wait_recv()

        @pl.when(d < last)
        def _():
            v_copy(above, vd_send.at[d], at_z(-1)).start()
            v_copy(below, vu_send.at[0], at_z(1)).wait_recv()

        @pl.when(d < last - 1)
        def _():
            v_copy(below, vu_send.at[d], at_z(1)).start()

    pass_keys(1)

    for i in (1, 3, 2):
        block = lax.rem(y + i, NY)
        remote(qbuf.at[block], qbuf.at[block], q_send.at[0], q_recv.at[block], at_y(1)).wait_recv()
        blocked(block)

    pass_values(1)

    @pl.when(y < NY - 1)
    def _():
        s_ref[0] = scores(z, y + 1)

        @pl.loop(y + 1, NY)
        def _(block):
            s_ref[1] = scores(z, NY + block)
            absorb(z, block, s_ref[0])
            s_ref[0] = scores(z, lax.rem(block + 1, NY))
            absorb(z, NY + block, s_ref[1])

    tail.wait_recv()
    rim = f32(tail_in[8:])
    cpad[:8] = jnp.where(sp > 0, rim, jnp.zeros_like(rim))
    summed = taps[0:1] * cpad[6 : 6 + ROWS]
    summed += taps[1:2] * cpad[7 : 7 + ROWS]
    summed += taps[2:3] * cpad[8 : 8 + ROWS]
    convg[tp] = bf16(ogate[...] * summed)
    conv.start(0)

    def half_block(source, g):
        @pl.when(source < z)
        def _():
            four_tiles(source, g)

    @pl.loop(0, NZ - 2)
    def _(i):
        d, r = i // 2 + 1, lax.rem(i, 2)
        source = lax.rem(z + jnp.where(r == 0, NZ - d, d), NZ)

        half_block(source, 0)

        @pl.when(r == 0)
        def _():
            pass_keys(d + 1)

        @pl.when(r == 1)
        def _():
            pass_values(d + 1)

        half_block(source, 1)

        @pl.when(i == 1)
        def _():
            conv.neighbours_first(0)
            conv.neighbours_second(0)

        @pl.when(i == 3)
        def _():
            conv.opposite(0, 1)

    def st_copy(h, i):
        return remote(stg.at[y, h], stg.at[y, h], st_send.at[h, i - 1], st_recv.at[y, h], at_y(i))

    for h in (0, 1):
        half_block(lax.rem(z + last, NZ), h)
        for t in range(NY):
            stg[y, h, t : t + 1] = m_ref[h * NY + t]
            stg[y, h, NY + t : NY + t + 1] = a_ref[h * NY + t, VDIM : VDIM + 1]
        for i in (2, 1, 3):
            st_copy(h, i).start()

    for load in loads[6:]:
        load.wait()
    for dx, h in ((-1, 0), (1, 1), (-1, 1), (1, 0), (0, 0), (0, 1), (2, 0), (2, 1)):
        conv.wait(dx, True, h)

    def mixed(buf, which, slot, rows):
        return jnp.dot(buf[slot, rows], obuf[which, slot], preferred_element_type=jnp.float32)

    oacc[...] = mixed(convg, 1, 0, slice(0, ROWS))

    @pl.loop(1, NTP)
    def _(slot):
        oacc[...] += mixed(convg, 1, slot, slice(0, ROWS))

    to = (at_y(1), at_y(3))
    near = (lax.rem(y + 1, NY), lax.rem(y + 3, NY))
    opposite = lax.rem(y + 2, NY)
    second = lax.broadcasted_iota(jnp.int32, (NY, LANES), 1) >= TILE

    def combined(h, block):
        part = a_ref[h * NY + block, :VDIM] * coef[h, pl.ds(block, 1)]
        return part[:, :TILE] + part[:, TILE:]

    def part_copy(h, k, target, device):
        n = 3 * h + k
        return remote(csend.at[n], target, c_send.at[n], c_recv.at[n], device)

    c_copies = [
        [
            part_copy(h, 0, crelay.at[h], to[h]),
            part_copy(h, 1, crecv.at[h, 0], to[1 - h]),
            part_copy(h, 2, crecv.at[h, 1], to[h]),
        ]
        for h in (0, 1)
    ]

    def weigh(h):
        for i in (1, 3, 2):
            peer = lax.rem(y + i, NY)
            remote(
                stg.at[peer, h], stg.at[peer, h], st_send.at[h, 0], st_recv.at[peer, h], at_y(1)
            ).wait_recv()
        m_all = stg[0, h, :NY]
        for i in range(1, NY):
            m_all = jnp.maximum(m_all, stg[i, h, :NY])
        l_all = stg[0, h, NY:] * jnp.exp2(stg[0, h, :NY] - m_all)
        for i in range(1, NY):
            l_all = l_all + stg[i, h, NY:] * jnp.exp2(stg[i, h, :NY] - m_all)
        share = jnp.exp2(stg[y, h, :NY] - m_all) / l_all
        coef[h, :NY] = jnp.where(second, -lam[0] * share, share)
        coef[h, NY:] = m_all * LN2 + jnp.log(l_all)
        csend[3 * h] = bf16(combined(h, opposite))
        c_copies[h][0].start()
        csend[3 * h + 1] = bf16(combined(h, near[1 - h]))
        c_copies[h][1].start()
        cown[:, h * TILE : (h + 1) * TILE] = combined(h, near[h])

    def pass_on(h):
        lanes = slice(h * TILE, (h + 1) * TILE)
        c_copies[h][0].wait_recv()
        csend[3 * h + 2] = bf16(cown[:, lanes] + f32(crelay[h]))
        c_copies[h][2].start()
        cown[:, lanes] = combined(h, y)
        row = coef[h, pl.ds(NY + y, 1)]
        logs[0, 0:1, lanes] = row[:, :TILE]
        logs[0, 1:2, lanes] = row[:, TILE:]

    def settle(h):
        c_copies[h][1].wait_recv()
        c_copies[h][2].wait_recv()
        head_mix = cown[:, h * TILE : (h + 1) * TILE] + f32(crecv[h, 0]) + f32(crecv[h, 1])
        mean = jnp.sum(head_mix * head_mix, axis=0, keepdims=True) / VDIM
        normed = jnp.transpose(head_mix * lax.rsqrt(mean + HEAD_EPS))
        attng[tp, h * HALF : (h + 1) * HALF] = bf16(normed * head_gain[...] * HEAD_SCALE)
        attn.start(2 * h)

    for stage in (weigh, pass_on, settle):
        for h in (0, 1):
            stage(h)

    def add(slot, h):
        rows = slice(h * HALF, (h + 1) * HALF)
        oacc[rows] += mixed(attng, 0, slot, rows)

    add(tp, 0)
    add(tp, 1)
    gathered(attn, add)
    out[...] = bf16(oacc[...])

    tokens.finish()
    for d in range(NZ // 2):
        k_copy(z, ku_send.at[d], at_z(1)).wait_send()
        v_copy(z, vd_send.at[d], at_z(-1)).wait_send()
        if d < NZ // 2 - 1:
            k_copy(z, kd_send.at[d], at_z(-1)).wait_send()
            v_copy(z, vu_send.at[d], at_z(1)).wait_send()
    for copy in q_copies + c_copies[0] + c_copies[1] + [tail]:
        copy.wait_send()
    for h in (0, 1):
        for i in (1, 2, 3):
            st_copy(h, i).wait_send()
    conv.finish()
    attn.finish()


def per_device(
    tokens,
    norm_gain,
    query_weight,
    key_weight,
    value_weight,
    outer_gate_weight,
    inner_gate_weight,
    conv_input_weight,
    conv_taps,
    lambdas,
    head_gain,
    attn_out_weight,
    conv_out_weight,
):
    half = DIM // 2
    frequency = np.float32(ROPE_BASE) ** (-np.arange(half, dtype=np.float32) * 2.0 / DIM)
    frequency = np.tile(frequency.astype(np.float64), 4)
    sign = np.tile(np.repeat([-1.0, 1.0], half), 2)
    start = np.arange(NY * NZ)[:, None] * ROWS * frequency
    cosine, sine = np.cos(start), np.sin(start)
    base = np.stack([cosine, sine, sign * cosine, sign * sine], axis=1).astype(np.float32)
    row = np.arange(ROWS)[:, None] * frequency
    rows = np.stack([np.cos(row), np.sin(row)]).astype(np.float32)

    def in_pieces(weight):
        return weight.reshape(NTP, PIECE, VDIM)

    vmem = pl.BlockSpec(memory_space=pltpu.VMEM)
    anywhere = pl.BlockSpec(memory_space=pltpu.HBM)
    dma = pltpu.SemaphoreType.DMA
    bf, fl = jnp.bfloat16, jnp.float32
    mixed_out, logs = pl.pallas_call(
        kernel,
        out_shape=(
            jax.ShapeDtypeStruct((ROWS, PIECE), bf),
            jax.ShapeDtypeStruct((1, 2, ROWS), fl),
        ),
        in_specs=[anywhere] * 15,
        out_specs=(vmem, vmem),
        scratch_shapes=[
            pltpu.VMEM((ROWS, PIECE), bf),
            pltpu.VMEM((NTP, 1, PIECE), fl),
            pltpu.VMEM((4, 128), fl),
            pltpu.VMEM((2, ROWS, 128), fl),
            pltpu.VMEM((3, VDIM), fl),
            pltpu.SMEM((1,), fl),
            pltpu.VMEM((1, VDIM), fl),
            pltpu.VMEM((NTP, ROWS, PIECE), bf),
            pltpu.VMEM((NTP, PIECE, 6 * VDIM), bf),
            pltpu.VMEM((2, NTP, VDIM, PIECE), bf),
            pltpu.VMEM((ROWS, 6 * VDIM), fl),
            pltpu.VMEM((ROWS, 128), fl),
            pltpu.VMEM((NZ, ROWS, VDIM), bf),
            pltpu.VMEM((NZ, VDIM, ROWS), bf),
            pltpu.VMEM((NY, VDIM, ROWS), bf),
            pltpu.VMEM((TILES, 2 * VDIM, LANES), bf),
            pltpu.VMEM((TILES, 1, LANES), fl),
            pltpu.VMEM((TILES, VDIM + ONES_ROWS, LANES), fl),
            pltpu.VMEM((2, ROWS, LANES), fl),
            pltpu.VMEM((NY, 2, TILES, LANES), fl),
            pltpu.VMEM((2, TILES, LANES), fl),
            pltpu.VMEM((6, VDIM, TILE), bf),
            pltpu.VMEM((2, VDIM, TILE), bf),
            pltpu.VMEM((2, 2, VDIM, TILE), bf),
            pltpu.VMEM((VDIM, ROWS), fl),
            pltpu.VMEM((ROWS, VDIM), fl),
            pltpu.VMEM((8 + ROWS, VDIM), fl),
            pltpu.VMEM((16, VDIM), bf),
            pltpu.VMEM((16, VDIM), bf),
            pltpu.VMEM((NTP, ROWS, VDIM), bf),
            pltpu.VMEM((NTP, ROWS, VDIM), bf),
            pltpu.VMEM((ROWS, PIECE), fl),
            dma((8,)),
            dma((7,)),
            dma((14,)),
            dma((NTP, 2)),
            dma((NZ // 2,)),
            dma((NZ // 2,)),
            dma((NZ // 2,)),
            dma((NZ // 2,)),
            dma((NZ,)),
            dma((NZ,)),
            dma((NY,)),
            dma((NY,)),
            dma((2, NY)),
            dma((NY, 2)),
            dma((6,)),
            dma((6,)),
            dma,
            dma,
            dma((14,)),
            dma((NTP, 2)),
            dma((28,)),
            dma((NTP, 4)),
        ],
        compiler_params=pltpu.CompilerParams(
            collective_id=0, has_side_effects=True, vmem_limit_bytes=40 * 2**20
        ),
    )(*(v if v is lambdas else pltpu.with_memory_space_constraint(v, pltpu.HBM) for v in (
        tokens,
        norm_gain.reshape(NTP, 1, PIECE),
        *(
            in_pieces(w)
            for w in (
                query_weight,
                key_weight,
                value_weight,
                outer_gate_weight,
                inner_gate_weight,
                conv_input_weight,
            )
        ),
        jnp.asarray(base),
        jnp.asarray(rows),
        conv_taps,
        lambdas,
        head_gain.reshape(1, VDIM),
        attn_out_weight.reshape(NTP, VDIM, PIECE),
        conv_out_weight.reshape(NTP, VDIM, PIECE),
    )))
    return mixed_out, logs


def solution(mesh):
    in_specs = (
        P("sp", "tp"),
        P(),
        P(None, "tp"),
        P(None, "tp"),
        P(None, "tp"),
        P(None, "tp"),
        P(None, "tp"),
        P(None, "tp"),
        P(None, "tp"),
        P("tp"),
        P(),
        P(None, "tp"),
        P(None, "tp"),
    )
    out_specs = (P("sp", "tp"), P("tp", None, "sp"))
    return jax.shard_map(
        per_device, mesh=mesh, in_specs=in_specs, out_specs=out_specs, check_vma=False
    )
```
